32 devices in a mesh: ep: 32 (over z, y, x, core).
Axes of the slice: x: 2, y: 2, z: 4, core: 2. Of those that a mesh axis runs over, the one named last changes fastest.
Arguments:
- tokens: bfloat16 [32, 2048], P('ep'), may hold values from -6 to 6
- mixer_gain: float32 [2048], replicated, may hold values from 0.1 to 1.9
- query_weight: bfloat16 [2048, 2048], P(None, 'ep'), may hold values from -0.125 to 0.125
- key_weight: bfloat16 [2048, 2048], P(None, 'ep'), may hold values from -0.125 to 0.125
- value_weight: bfloat16 [2048, 2048], P(None, 'ep'), may hold values from -0.125 to 0.125
- outgate_weight: bfloat16 [2048, 2048], P(None, 'ep'), may hold values from -0.125 to 0.125
- input_weight: bfloat16 [2048, 4], replicated, may hold values from -0.125 to 0.125
- forget_weight: bfloat16 [2048, 4], replicated, may hold values from -0.125 to 0.125
- forget_bias: float32 [4], replicated, may hold values from 0 to 4
- memory_matrix: float32 [32, 4, 512, 512], P('ep'), may hold values from -0.3 to 0.3
- memory_norm: float32 [32, 4, 512], P('ep'), may hold values from -0.3 to 0.3
- memory_max: float32 [32, 4], P('ep'), may hold values from -2 to 2
- mixer_out: bfloat16 [2048, 2048], P(None, 'ep'), may hold values from -0.125 to 0.125
- expert_gain: float32 [2048], replicated, may hold values from 0.1 to 1.9
- expert_gate: bfloat16 [32, 2048, 1024], P('ep'), may hold values from -0.125 to 0.125
- expert_up: bfloat16 [32, 2048, 1024], P('ep'), may hold values from -0.125 to 0.125
- expert_down: bfloat16 [32, 1024, 2048], P('ep'), may hold values from -0.1875 to 0.1875
- route_group: int32 [32], P('ep'), may hold values from 0 to 3
- route_member: int32 [32, 2], P('ep'), may hold values from 0 to 7, as said below
- group_weight: float32 [32], P('ep'), may hold values from 0.25 to 1
- member_weight: float32 [32, 2], P('ep'), may hold values from 0.1 to 1
Outputs:
- layer_out: bfloat16 [32, 2048], P('ep')
- next_matrix: float32 [32, 4, 512, 512], P('ep')
- next_norm: float32 [32, 4, 512], P('ep')
- next_max: float32 [32, 4], P('ep')
The draws below stay inside these ranges and needn't reach their ends.
Inputs may be any that keep to these rules, and one draw needn't show every extreme that they name: A row's 2 experts, numbered route_group * 8 + route_member, are different members of the one group that route_group names. No expert is named by more than 4 rows in all, and one expert is named by exactly 4 rows.
All inputs are finite; a program needn't handle non-finite values.
Results may differ from the reference program's by a relative error of at most 0.013.
Values may be sent and summed in bfloat16 or wider, within the bound.
No kernel may reach another device: no remote copies, remote signals or barrier semaphores. Data moves between devices by JAX's collectives and lax.ppermute only.
A program may use at most 64 MiB of HBM per device.

```python
import math
import jax
import jax.numpy as jnp
from jax import lax

D = 2048
HEADS = 4
HEAD_DIM = 512
FF = 1024
GROUPS = 4
TOP_K = 2
SEQ_DEV = 1
TOKENS = 32
EXPERTS = 32
MEMBERS = 8
CAPACITY = 4


def route_tables(key):
    base = jax.random.fold_in(key, 11)
    streams = jax.random.split(base, 4)
    favour = jax.random.randint(streams[0], (EXPERTS,), 0, 64)
    hottest = jax.random.randint(streams[1], (), 0, EXPERTS)
    noise = jax.random.randint(streams[2], (TOKENS, EXPERTS), 0, 64)
    column = jnp.arange(EXPERTS, dtype=jnp.int32)
    row_index = jnp.arange(TOKENS, dtype=jnp.int32)
    score = noise + 2 * favour[None, :] + jnp.where(column == hottest, 4096, 0)[None, :]
    forced = jnp.where((row_index[:, None] == 0) & (column[None, :] == EXPERTS // 2), 16384, 0)
    forced = forced + jnp.where((row_index[:, None] == SEQ_DEV) & (column[None, :] == 0), 16384, 0)
    score = (score + forced) * EXPERTS + column[None, :]
    ranking = jax.random.permutation(streams[3], TOKENS).astype(jnp.int32)
    ranking = jnp.where(row_index == 0, -2, jnp.where(row_index == SEQ_DEV, -1, ranking))
    order = jnp.argsort(ranking).astype(jnp.int32)

    def visit(load, row):
        open_slots = load < CAPACITY
        masked = jnp.where(open_slots, score[row], -1)
        counts = jnp.sum(open_slots.reshape(GROUPS, MEMBERS).astype(jnp.int32), axis=1)
        best = jnp.where(counts >= TOP_K, jnp.max(masked.reshape(GROUPS, MEMBERS), axis=1), -1 - jnp.arange(GROUPS, dtype=jnp.int32))
        group_pick = lax.top_k(best, 1)[1][0].astype(jnp.int32)
        inside = lax.dynamic_slice_in_dim(masked, group_pick * MEMBERS, MEMBERS)
        picks = lax.top_k(inside, TOP_K)[1].astype(jnp.int32)
        load = load.at[group_pick * MEMBERS + picks].add(1)
        return (load, (group_pick, picks))
    _, (groups_seen, members_seen) = lax.scan(visit, jnp.zeros((EXPERTS,), jnp.int32), order)
    group_ids = jnp.zeros((TOKENS,), jnp.int32).at[order].set(groups_seen)
    member_ids = jnp.zeros((TOKENS, TOP_K), jnp.int32).at[order].set(members_seen)
    return (group_ids, member_ids)


def draw_route_group(key, part):
    return route_tables(key)[0]


def draw_route_member(key, part):
    return route_tables(key)[1]


def steps_of(key, shape, pieces, smallest, top_value):
    def one(position, blocks):
        steps = jax.random.uniform(jax.random.fold_in(jax.random.fold_in(key, 6), position), (blocks,), jnp.float32, smallest / len(pieces), top_value / len(pieces))
        return jnp.repeat(jnp.exp(steps), shape[position] // blocks).reshape((-1,) + (1,) * (len(shape) - position - 1))

    loudness = one(*pieces[0])
    for cut in pieces[1:]:
        loudness = loudness * one(*cut)
    return loudness


def scatter_about(rng, extent, width, reach, cuts=(), kind=jnp.bfloat16):
    level = steps_of(rng, extent, cuts, -0.22, 0.18) if cuts else 1.0
    drawn = jax.random.normal(rng, extent, jnp.float32) * width * level
    return jnp.minimum(jnp.maximum(drawn, -reach), reach).astype(kind)


def setup_inputs(seed: int = 0) -> dict:
    arg_keys = jax.random.split(jax.random.key(seed), 22)
    return {
        "tokens": scatter_about(arg_keys[0], (TOKENS, D), 1.0, 6.0, ((0, 32),)),
        "mixer_gain": jnp.clip(1.0 + 0.18 * jax.random.normal(arg_keys[1], (D,), jnp.float32), 0.1, 1.9),
        "query_weight": scatter_about(arg_keys[2], (D, D), D ** -0.5, 0.125, ((1, 32),)),
        "key_weight": scatter_about(arg_keys[3], (D, D), D ** -0.5, 0.125, ((1, 32),)),
        "value_weight": scatter_about(arg_keys[4], (D, D), D ** -0.5, 0.125, ((1, 32),)),
        "outgate_weight": scatter_about(arg_keys[5], (D, D), D ** -0.5, 0.125, ((1, 32),)),
        "input_weight": scatter_about(arg_keys[6], (D, HEADS), D ** -0.5, 0.125),
        "forget_weight": scatter_about(arg_keys[7], (D, HEADS), D ** -0.5, 0.125),
        "forget_bias": jnp.clip(jax.random.uniform(arg_keys[8], (HEADS,), jnp.float32, 0.0, 4.0), 0.0, 4.0),
        "memory_matrix": scatter_about(arg_keys[9], (TOKENS, HEADS, HEAD_DIM, HEAD_DIM), 0.05, 0.3, ((0, 32),), jnp.float32),
        "memory_norm": scatter_about(arg_keys[10], (TOKENS, HEADS, HEAD_DIM), 0.05, 0.3, ((0, 32),), jnp.float32),
        "memory_max": jnp.clip(jax.random.uniform(arg_keys[11], (TOKENS, HEADS), jnp.float32, -2.0, 2.0) * steps_of(arg_keys[11], (TOKENS, HEADS), ((0, 32),), -0.4, 0.0), -2.0, 2.0),
        "mixer_out": scatter_about(arg_keys[12], (D, D), D ** -0.5, 0.125, ((1, 32),)),
        "expert_gain": jnp.clip(1.0 + 0.18 * jax.random.normal(arg_keys[13], (D,), jnp.float32), 0.1, 1.9),
        "expert_gate": scatter_about(arg_keys[14], (EXPERTS, D, FF), D ** -0.5, 0.125, ((0, 32),)),
        "expert_up": scatter_about(arg_keys[15], (EXPERTS, D, FF), D ** -0.5, 0.125, ((0, 32),)),
        "expert_down": scatter_about(arg_keys[16], (EXPERTS, FF, D), FF ** -0.5, 0.1875, ((0, 32),)),
        "route_group": draw_route_group(jax.random.fold_in(arg_keys[21], 71), 0),
        "route_member": draw_route_member(jax.random.fold_in(arg_keys[21], 71), 0),
        "group_weight": jnp.clip(jnp.exp(math.log(1.0) - 1.3862944 * jax.random.uniform(arg_keys[19], (TOKENS,), jnp.float32) ** steps_of(arg_keys[19], (TOKENS,), ((0, 32),), -0.2, 0.2)), 0.25, 1.0),
        "member_weight": jnp.clip(jnp.exp(math.log(1.0) - 2.3025851 * jax.random.uniform(arg_keys[20], (TOKENS, TOP_K), jnp.float32) ** steps_of(arg_keys[20], (TOKENS, TOP_K), ((0, 32),), -0.2, 0.2)), 0.1, 1.0),
    }


norm_eps = 1e-06

def root_norm(values, gain):
    return values * lax.rsqrt(lax.optimization_barrier(jnp.mean(values * values, axis=-1, keepdims=True)) + norm_eps) * gain

def reference(tokens, mixer_gain, query_weight, key_weight, value_weight, outgate_weight, input_weight, forget_weight, forget_bias, memory_matrix, memory_norm, memory_max, mixer_out, expert_gain, expert_gate, expert_up, expert_down, route_group, route_member, group_weight, member_weight):
    count = tokens.shape[0]
    resid = tokens.astype(jnp.float32)
    normed = root_norm(resid, mixer_gain).astype(jnp.bfloat16)
    query = jnp.dot(normed, query_weight, preferred_element_type=jnp.float32).astype(jnp.bfloat16)
    key = jnp.dot(normed, key_weight, preferred_element_type=jnp.float32).astype(jnp.bfloat16)
    value = jnp.dot(normed, value_weight, preferred_element_type=jnp.float32).astype(jnp.bfloat16)
    outgate = jnp.dot(normed, outgate_weight, preferred_element_type=jnp.float32).astype(jnp.bfloat16)
    input_pre = jnp.dot(normed, input_weight, preferred_element_type=jnp.float32)
    forget_pre = jnp.dot(normed, forget_weight, preferred_element_type=jnp.float32) + forget_bias
    log_forget = jax.nn.log_sigmoid(forget_pre)
    next_max = jnp.maximum(log_forget + memory_max, input_pre)
    keep = jnp.exp(log_forget + memory_max - next_max)
    admit = jnp.exp(input_pre - next_max)
    query_heads = query.astype(jnp.float32).reshape(count, HEADS, HEAD_DIM)
    key_heads = key.astype(jnp.float32).reshape(count, HEADS, HEAD_DIM) * HEAD_DIM ** (-0.5)
    value_heads = value.astype(jnp.float32).reshape(count, HEADS, HEAD_DIM)
    carried = jnp.einsum('shij,shj->shi', memory_matrix, query_heads, precision=lax.Precision.HIGHEST)
    score = lax.optimization_barrier(jnp.sum(key_heads * query_heads, axis=-1))
    numer = keep[..., None] * carried + (admit * score)[..., None] * value_heads
    denom = keep * lax.optimization_barrier(jnp.sum(memory_norm * query_heads, axis=-1)) + admit * score
    head_out = numer / jnp.maximum(jnp.abs(denom), jnp.exp(-next_max))[..., None]
    gated = (head_out.reshape(count, D) * jax.nn.sigmoid(outgate.astype(jnp.float32))).astype(jnp.bfloat16)
    next_matrix = keep[..., None, None] * memory_matrix + admit[..., None, None] * value_heads[..., :, None] * key_heads[..., None, :]
    next_norm = keep[..., None] * memory_norm + admit[..., None] * key_heads
    projected = jnp.dot(gated, mixer_out, preferred_element_type=jnp.float32).astype(jnp.bfloat16)
    middle = (resid + projected.astype(jnp.float32)).astype(jnp.bfloat16)
    expert_in = root_norm(middle.astype(jnp.float32), expert_gain).astype(jnp.bfloat16)
    chosen = (route_group[:, None] * MEMBERS + route_member).astype(jnp.int32)
    slot_rows = jnp.repeat(jnp.arange(count, dtype=jnp.int32), TOP_K)

    def one_slot(pair):
        row_index, expert_index = pair
        row = lax.dynamic_slice_in_dim(expert_in, row_index, 1, 0)
        gate_part = jnp.dot(row, expert_gate[expert_index], preferred_element_type=jnp.float32)
        up_part = jnp.dot(row, expert_up[expert_index], preferred_element_type=jnp.float32)
        hidden = (jax.nn.silu(gate_part) * up_part).astype(jnp.bfloat16)
        return jnp.dot(hidden, expert_down[expert_index], preferred_element_type=jnp.float32).astype(jnp.bfloat16)[0]
    results = lax.map(one_slot, (slot_rows, chosen.reshape(-1))).reshape(count, TOP_K, D)
    weight = group_weight[:, None] * member_weight
    mixture = lax.optimization_barrier(jnp.sum(weight[..., None] * results.astype(jnp.float32), axis=1))
    layer_out = (middle.astype(jnp.float32) + mixture).astype(jnp.bfloat16)
    return (layer_out, next_matrix, next_norm, next_max)
```

```python
import jax
import jax.numpy as jnp
from jax import lax
from jax.sharding import PartitionSpec as P

GROUPS = 4
CAPACITY = 4
LANES = 128


norm_eps = 1e-06


def root_norm(values, gain):
    return values * lax.rsqrt(jnp.mean(values * values, axis=-1, keepdims=True) + norm_eps) * gain


def run_expert(slot_rows, gate_mat, up_mat, down_mat):
    gate_part = jnp.dot(slot_rows, gate_mat, preferred_element_type=jnp.float32)
    up_part = jnp.dot(slot_rows, up_mat, preferred_element_type=jnp.float32)
    hidden = (jax.nn.silu(gate_part) * up_part).astype(jnp.bfloat16)
    return jnp.dot(hidden, down_mat, preferred_element_type=jnp.float32).astype(jnp.bfloat16)


def exchange(blocks):
    return lax.all_to_all(blocks, "ep", split_axis=0, concat_axis=0, tiled=True)


def local(
    tokens,
    mixer_gain,
    query_weight,
    key_weight,
    value_weight,
    outgate_weight,
    input_weight,
    forget_weight,
    forget_bias,
    memory_matrix,
    memory_norm,
    memory_max,
    mixer_out,
    expert_gain,
    expert_gate,
    expert_up,
    expert_down,
    route_group,
    route_member,
    group_weight,
    member_weight,
):
    devices = lax.axis_size("ep")
    width = tokens.shape[1]
    columns = query_weight.shape[1]
    heads = memory_matrix.shape[1]
    head_dim = memory_matrix.shape[2]
    members = devices // GROUPS
    picks = route_member.shape[1]
    assert tokens.shape[0] == 1 and expert_gate.shape[0] == 1

    route = jnp.concatenate([route_group[:, None], route_member], axis=1).astype(jnp.bfloat16)
    route = jnp.pad(route, ((0, 0), (0, 2 * LANES - 1 - picks)))
    row = jnp.concatenate([tokens, route], axis=1)
    gathered = exchange(jnp.broadcast_to(row, (devices, row.shape[1])))
    rows = gathered[:, :width]
    ids = gathered[:, width:width + 1 + picks].astype(jnp.int32)
    chosen = ids[:, :1] * members + ids[:, 1:]

    targets = jnp.arange(devices, dtype=jnp.int32)
    hit = jnp.any(chosen[:, :, None] == targets[None, None, :], axis=1)
    hit_bf = hit.astype(jnp.bfloat16)
    upto = (targets[:, None] <= targets[None, :]).astype(jnp.bfloat16)
    place = jnp.dot(hit_bf.T, upto, preferred_element_type=jnp.float32) - 1.0
    slots = jnp.arange(CAPACITY, dtype=jnp.float32)
    take = hit.T[:, None, :] & (place[:, None, :] == slots[None, :, None])
    own = (targets[:, None] == targets[None, :])[:, None, :]
    take = jnp.concatenate([take, own], axis=1).astype(jnp.bfloat16)

    stacked = jnp.concatenate([query_weight, key_weight, value_weight, outgate_weight], axis=1)
    normed = root_norm(rows.astype(jnp.float32), mixer_gain).astype(jnp.bfloat16)
    result = jnp.dot(normed, stacked, preferred_element_type=jnp.float32).astype(jnp.bfloat16)
    parts = exchange(result).reshape(devices, 4, columns).transpose(1, 0, 2).reshape(4, heads, head_dim)

    resid = tokens.astype(jnp.float32)
    own_normed = root_norm(resid, mixer_gain).astype(jnp.bfloat16)
    input_pre = jnp.dot(own_normed, input_weight, preferred_element_type=jnp.float32)
    forget_pre = (
        jnp.dot(own_normed, forget_weight, preferred_element_type=jnp.float32) + forget_bias
    )
    log_forget = jax.nn.log_sigmoid(forget_pre)
    next_max = jnp.maximum(log_forget + memory_max, input_pre)
    keep = jnp.exp(log_forget + memory_max - next_max)
    admit = jnp.exp(input_pre - next_max)

    parts = parts.astype(jnp.float32)
    query_heads = parts[0][None]
    key_heads = parts[1][None] * head_dim ** (-0.5)
    value_heads = parts[2][None]
    carried = jnp.einsum(
        "shij,shj->shi", memory_matrix, query_heads, precision=lax.Precision.HIGHEST
    )
    score = jnp.sum(key_heads * query_heads, axis=-1)
    numer = keep[..., None] * carried + (admit * score)[..., None] * value_heads
    denom = keep * jnp.sum(memory_norm * query_heads, axis=-1) + admit * score
    head_out = numer / jnp.maximum(jnp.abs(denom), jnp.exp(-next_max))[..., None]
    gated = (head_out * jax.nn.sigmoid(parts[3][None])).reshape(1, width).astype(jnp.bfloat16)
    next_matrix = (
        keep[..., None, None] * memory_matrix
        + admit[..., None, None] * value_heads[..., :, None] * key_heads[..., None, :]
    )
    next_norm = keep[..., None] * memory_norm + admit[..., None] * key_heads

    gated_rows = exchange(jnp.broadcast_to(gated, (devices, width)))

    proj_cols = jnp.dot(gated_rows, mixer_out, preferred_element_type=jnp.float32).astype(jnp.bfloat16)
    outgoing = jnp.dot(
        take.reshape(devices * (CAPACITY + 1), devices), proj_cols, preferred_element_type=jnp.float32
    ).astype(jnp.bfloat16)
    incoming = exchange(outgoing.reshape(devices, (CAPACITY + 1) * columns))
    projected = incoming.reshape(devices, CAPACITY + 1, columns).transpose(1, 0, 2)
    projected = projected.reshape(CAPACITY + 1, width).astype(jnp.float32)
    me = lax.axis_index("ep")
    mine = lax.dynamic_index_in_dim(take, me, axis=0, keepdims=False)
    slot_resid = jnp.dot(mine, rows, preferred_element_type=jnp.float32)
    middle = (slot_resid + projected).astype(jnp.bfloat16)
    expert_in = root_norm(middle[:CAPACITY].astype(jnp.float32), expert_gain).astype(jnp.bfloat16)
    finished = run_expert(expert_in, expert_gate[0], expert_up[0], expert_down[0])

    back_rows = jnp.dot(
        mine[:CAPACITY].T, finished, preferred_element_type=jnp.float32
    ).astype(jnp.bfloat16)
    returned = exchange(back_rows)
    local_chosen = route_group[:, None] * members + route_member
    local_weight = group_weight[:, None] * member_weight
    weights = jnp.sum(
        jnp.where(local_chosen[:, :, None] == targets[None, None, :], local_weight[:, :, None], 0.0), axis=1
    )
    mixture = jnp.sum(weights.T * returned.astype(jnp.float32), axis=0, keepdims=True)
    layer_out = (middle[CAPACITY:].astype(jnp.float32) + mixture).astype(jnp.bfloat16)
    return (layer_out, next_matrix, next_norm, next_max)


def solution(mesh):
    placed = (
        P("ep", None),
        P(),
        P(None, "ep"),
        P(None, "ep"),
        P(None, "ep"),
        P(None, "ep"),
        P(),
        P(),
        P(),
        P("ep", None, None, None),
        P("ep", None, None),
        P("ep", None),
        P(None, "ep"),
        P(),
        P("ep", None, None),
        P("ep", None, None),
        P("ep", None, None),
        P("ep"),
        P("ep", None),
        P("ep"),
        P("ep", None),
    )
    return jax.shard_map(
        local,
        mesh=mesh,
        in_specs=placed,
        out_specs=(P("ep", None), P("ep", None, None, None), P("ep", None, None), P("ep", None)),
        check_vma=False,
    )
```

```python
import jax
import jax.numpy as jnp
from jax import lax
from jax.experimental import pallas as pl
from jax.experimental.pallas import tpu as pltpu
from jax.sharding import PartitionSpec as P

GROUPS = 4
CAPACITY = 4
LANES = 128
SLOTS = 8
MIB = 1 << 20
F32 = jnp.float32
BF16 = jnp.bfloat16
NT = (((1,), (1,)), ((), ()))


norm_eps = 1e-06


def root_norm(values, gain):
    return values * lax.rsqrt(jnp.mean(values * values, axis=-1, keepdims=True) + norm_eps) * gain


def exchange(blocks):
    count, width = blocks.shape
    halves = blocks.reshape(count, 2, width // 2)
    return lax.all_to_all(halves, "ep", split_axis=0, concat_axis=0, tiled=True).reshape(count, width)


VMEM_SPEC = pl.BlockSpec(memory_space=pltpu.VMEM)
SMEM_SPEC = pl.BlockSpec(memory_space=pltpu.SMEM)
HBM_SPEC = pl.BlockSpec(memory_space=pltpu.HBM)


def call(body, outs, ins, scratch=(), limit=8 * MIB, flops=10_000_000, moved=1_000_000):
    return pl.pallas_call(
        body,
        out_shape=outs,
        in_specs=ins,
        out_specs=jax.tree.map(lambda _: VMEM_SPEC, outs),
        scratch_shapes=scratch,
        compiler_params=pltpu.CompilerParams(vmem_limit_bytes=limit),
        cost_estimate=pl.CostEstimate(flops=flops, bytes_accessed=moved, transcendentals=0),
    )


def in_hbm(array):
    return pltpu.with_memory_space_constraint(array, pltpu.HBM)


def shaped(shape, dtype=F32):
    return jax.ShapeDtypeStruct(shape, dtype)


def feature_rows(ref, offset, columns):
    group = LANES // columns
    count = ref.shape[1] // group
    tile, lane = divmod(offset, LANES)
    pieces = [
        ref[tile, pl.ds(g, count, stride=group), :][:, lane:lane + columns] for g in range(group)
    ]
    return jnp.concatenate(pieces, axis=1)


def spill(ref, values):
    for t in range(ref.shape[0]):
        part = values[:, t * LANES:(t + 1) * LANES]
        ref[t, :, :part.shape[1]] = part


def diagonal(n):
    i = lax.broadcasted_iota(jnp.int32, (n, n), 0)
    j = lax.broadcasted_iota(jnp.int32, (n, n), 1)
    return i == j


def to_column(row):
    n = row.shape[1]
    spread = jnp.broadcast_to(row, (n, n))
    return jnp.sum(jnp.where(diagonal(n), spread, 0.0), axis=1, keepdims=True)


def to_row(col):
    n = col.shape[0]
    spread = jnp.broadcast_to(col, (n, n))
    return jnp.sum(jnp.where(diagonal(n), spread, 0.0), axis=0, keepdims=True)


def fetch_columns_body(
    group_ref, member_ref, wq, wk, wv, wo, wi, wf, gain,
    stacked, wi_out, wf_out, gain_out, ids_out, sems,
):
    columns = wq.shape[0]
    copies = [
        pltpu.make_async_copy(w, stacked.at[pl.ds(n * columns, columns)], sems.at[n])
        for n, w in enumerate((wq, wk, wv, wo))
    ]
    copies += [
        pltpu.make_async_copy(a, b, sems.at[4 + n])
        for n, (a, b) in enumerate(((wi, wi_out), (wf, wf_out), (gain, gain_out)))
    ]
    for c in copies:
        c.start()
    lane = lax.broadcasted_iota(jnp.int32, ids_out.shape, 1)
    ids = jnp.where(lane == 0, group_ref[0], 0)
    for k in range(member_ref.shape[0]):
        ids = jnp.where(lane == 1 + k, member_ref[k], ids)
    ids_out[...] = ids.astype(F32)
    for c in copies:
        c.wait()


def fetch_cell_body(mem, norm, most, bias, mem_out, norm_out, most_out, bias_out, sems):
    early = mem_out.shape[0]
    copies = [
        pltpu.make_async_copy(a, b, sems.at[n])
        for n, (a, b) in enumerate(
            ((mem.at[pl.ds(0, early)], mem_out), (norm, norm_out), (most, most_out), (bias, bias_out))
        )
    ]
    for c in copies:
        c.start()
    for c in copies:
        c.wait()


def columns_body(rows_ref, ids_ref, gain_ref, stacked, wi, wf, out_ref, pre_ref):
    heads = wi.shape[0]
    count = rows_ref.shape[0]
    total = stacked.shape[0]
    normed = root_norm(rows_ref[...].astype(F32), gain_ref[...]).astype(BF16)
    cols = lax.dot_general(normed, stacked[...], NT, preferred_element_type=F32)
    out_ref[:, :total] = cols.astype(BF16)
    out_ref[:, total:] = jnp.broadcast_to(ids_ref[...], (count, ids_ref.shape[1])).astype(BF16)
    pre_ref[:heads, :] = lax.dot_general(wi[...], normed, NT, preferred_element_type=F32)
    pre_ref[heads:, :] = lax.dot_general(wf[...], normed, NT, preferred_element_type=F32)


def tables_body(
    me_ref, group_ref, member_ref, group_weight, member_weight, parts_ref,
    take_ref, mine_ref, spread_ref, weight_ref,
):
    count = parts_ref.shape[0]
    members = count // GROUPS
    picks = member_ref.shape[0]
    ids = parts_ref[:, parts_ref.shape[1] - LANES:].astype(F32)
    lane = lax.broadcasted_iota(jnp.int32, ids.shape, 1)

    def row_of(k):
        return to_row(jnp.sum(jnp.where(lane == k, ids, 0.0), axis=1, keepdims=True))

    group = row_of(0)
    expert = lax.broadcasted_iota(jnp.int32, (count, count), 0)
    token = lax.broadcasted_iota(jnp.int32, (count, count), 1)
    hit = jnp.zeros((count, count), F32)
    column = lax.broadcasted_iota(jnp.int32, (count, 1), 0)
    weight = jnp.zeros((count, 1), F32)
    for k in range(picks):
        chosen = (group * members + row_of(1 + k)).astype(jnp.int32)
        hit = jnp.where(expert == chosen, 1.0, hit)
        local = group_ref[0] * members + member_ref[k]
        weight += jnp.where(column == local, group_weight[0] * member_weight[k], 0.0)
    weight_ref[...] = weight
    upto = jnp.where(expert <= token, 1.0, 0.0).astype(BF16)
    place = jnp.dot(hit.astype(BF16), upto, preferred_element_type=F32)
    slot = lax.broadcasted_iota(jnp.int32, (SLOTS, count), 0)
    lane = lax.broadcasted_iota(jnp.int32, (count, SLOTS), 1)
    mine = jnp.zeros((SLOTS, count), F32)
    spread = jnp.zeros((count, SLOTS), F32)
    for s in range(CAPACITY + 1):
        if s < CAPACITY:
            take = jnp.where(place == s + 1.0, hit, 0.0)
        else:
            take = jnp.where(expert == token, 1.0, 0.0)
        take_ref[s] = take.astype(BF16)
        row = jnp.sum(jnp.where(expert == me_ref[0], take, 0.0), axis=0, keepdims=True)
        mine = jnp.where(slot == s, row, mine)
        if s < CAPACITY:
            spread = jnp.where(lane == s, to_column(row), spread)
    mine_ref[...] = mine.astype(BF16)
    spread_ref[...] = spread.astype(BF16)


def cell_body(
    me_ref, parts_ref, pre_ref, max_ref, bias_ref, norm_ref, early_ref, mem_ref,
    gated_ref, norm_out, max_out, value_out, key_out, keep_out,
    mem, wide, tall, sems,
):
    heads, head_dim = norm_ref.shape
    early = early_ref.shape[0]
    copies = [
        pltpu.make_async_copy(mem_ref.at[early + h], mem.at[h], sems.at[h]) for h in range(heads - early)
    ]
    for c in copies:
        c.start()

    columns = (parts_ref.shape[1] - LANES) // 4
    tiles = head_dim // LANES
    rows = heads * tiles
    spill(wide, parts_ref[:, :4 * columns].astype(F32))
    for n in range(4):
        tall[n * rows:(n + 1) * rows, :] = feature_rows(wide, n * columns, columns)

    def heads_of(n):
        return jnp.concatenate(
            [tall[pl.ds(n * rows + p, heads, stride=tiles), :] for p in range(tiles)], axis=1
        )

    query, key, value, outgate = (heads_of(n) for n in range(4))
    key = key * head_dim ** (-0.5)

    pre = pre_ref[...]
    lane = lax.broadcasted_iota(jnp.int32, pre.shape, 1)
    pre = jnp.sum(jnp.where(lane == me_ref[0], pre, 0.0), axis=1, keepdims=True)
    input_pre = pre[:heads]
    forget_pre = pre[heads:] + to_column(bias_ref[...])
    log_forget = jnp.minimum(forget_pre, 0.0) - jnp.log1p(jnp.exp(-jnp.abs(forget_pre)))
    carry = log_forget + to_column(max_ref[...])
    next_max = jnp.maximum(carry, input_pre)
    keep = jnp.exp(carry - next_max)
    admit = jnp.exp(input_pre - next_max)

    norm = norm_ref[...]
    score = admit * jnp.sum(key * query, axis=1, keepdims=True)
    denom = keep * jnp.sum(norm * query, axis=1, keepdims=True) + score
    scale = 1.0 / jnp.maximum(jnp.abs(denom), jnp.exp(-next_max))
    opened = jax.nn.sigmoid(outgate)
    norm_out[...] = keep * norm + admit * key
    max_out[...] = to_row(next_max)
    value_out[...] = admit * value
    key_out[...] = key
    keep_out[...] = jnp.broadcast_to(keep, keep_out.shape)

    count = gated_ref.shape[0]
    left = jnp.concatenate([query, jnp.zeros((8 - heads, head_dim), F32)], axis=0) if heads < 8 else query
    left = left.astype(BF16)
    for h in range(heads):
        if h < early:
            block = early_ref[h]
        else:
            copies[h - early].wait()
            block = mem[h - early]
        high = block.astype(BF16)
        low = (block - high.astype(F32)).astype(BF16)
        carried = lax.dot_general(left, high, NT, preferred_element_type=F32)
        carried = carried + lax.dot_general(left, low, NT, preferred_element_type=F32)
        carried = carried[h:h + 1]
        numer = keep[h:h + 1] * carried + score[h:h + 1] * value[h:h + 1]
        gated = numer * scale[h:h + 1] * opened[h:h + 1]
        gated_ref[:, h * head_dim:(h + 1) * head_dim] = jnp.broadcast_to(
            gated, (count, head_dim)
        ).astype(BF16)


def project_body(gated_ref, weight_ref, take_ref, out_ref):
    proj = lax.dot_general(gated_ref[...], weight_ref[...], NT, preferred_element_type=F32).astype(BF16)
    blocks = [
        jnp.dot(take_ref[s], proj, preferred_element_type=F32) for s in range(take_ref.shape[0])
    ]
    out_ref[...] = jnp.concatenate(blocks, axis=1).astype(BF16)


def expert_body(
    in_ref, rows_ref, mine_ref, spread_ref, gain_ref, gate_ref, up_ref, down_ref,
    out_ref, middle_ref,
    gate, up, down, wide, tall, sems,
):
    width, hidden_dim = gate_ref.shape
    steps = sems.shape[1]
    wide_step = width // steps
    tall_step = hidden_dim // steps
    plan = []
    for n, (src, dst, step) in enumerate(
        ((gate_ref, gate, wide_step), (up_ref, up, wide_step), (down_ref, down, tall_step))
    ):
        plan.append([
            pltpu.make_async_copy(
                src.at[pl.ds(k * step, step)], dst.at[pl.ds(k * step, step)], sems.at[n, k]
            )
            for k in range(steps)
        ])
    for k in range(steps):
        plan[0][k].start()
        plan[1][k].start()
    for k in range(steps):
        plan[2][k].start()

    used = CAPACITY + 1
    columns = in_ref.shape[1] // used
    tiles = width // LANES
    spill(wide, in_ref[...].astype(F32))
    for s in range(used):
        tall[s * tiles:(s + 1) * tiles, :] = feature_rows(wide, s * columns, columns)
    tall[used * tiles:, :] = jnp.zeros((tall.shape[0] - used * tiles, LANES), F32)
    projected = jnp.concatenate(
        [tall[pl.ds(r, SLOTS, stride=tiles), :] for r in range(tiles)], axis=1
    )
    resid = jnp.dot(mine_ref[...], rows_ref[...], preferred_element_type=F32)
    middle = (resid + projected).astype(BF16).astype(F32)
    middle_ref[...] = middle[CAPACITY:CAPACITY + 1]
    left = root_norm(middle, gain_ref[...]).astype(BF16)

    gate_part = jnp.zeros((SLOTS, hidden_dim), F32)
    up_part = jnp.zeros((SLOTS, hidden_dim), F32)
    for k in range(steps):
        part = slice(k * wide_step, (k + 1) * wide_step)
        plan[0][k].wait()
        gate_part += jnp.dot(left[:, part], gate[part, :], preferred_element_type=F32)
        plan[1][k].wait()
        up_part += jnp.dot(left[:, part], up[part, :], preferred_element_type=F32)
    hidden = (gate_part / (1.0 + jnp.exp(-gate_part)) * up_part).astype(BF16)
    result = jnp.zeros((SLOTS, width), F32)
    for k in range(steps):
        part = slice(k * tall_step, (k + 1) * tall_step)
        plan[2][k].wait()
        result += jnp.dot(hidden[:, part], down[part, :], preferred_element_type=F32)
    out_ref[...] = jnp.dot(
        spread_ref[...], result.astype(BF16), preferred_element_type=F32
    ).astype(BF16)


def finish_body(returned_ref, weight_ref, middle_ref, out_ref):
    mixture = jnp.sum(weight_ref[...] * returned_ref[...].astype(F32), axis=0, keepdims=True)
    out_ref[...] = (middle_ref[...] + mixture).astype(BF16)


def local(
    tokens,
    mixer_gain,
    query_weight,
    key_weight,
    value_weight,
    outgate_weight,
    input_weight,
    forget_weight,
    forget_bias,
    memory_matrix,
    memory_norm,
    memory_max,
    mixer_out,
    expert_gain,
    expert_gate,
    expert_up,
    expert_down,
    route_group,
    route_member,
    group_weight,
    member_weight,
):
    devices = lax.axis_size("ep")
    width = tokens.shape[1]
    columns = query_weight.shape[1]
    heads, head_dim = memory_norm.shape[1:]
    hidden_dim = expert_gate.shape[2]
    assert tokens.shape[0] == 1 and expert_gate.shape[0] == 1
    me = lax.axis_index("ep").astype(jnp.int32)

    ids = (route_group, route_member.reshape(-1))

    rows = exchange(jnp.broadcast_to(tokens, (devices, width)))

    stacked, wi, wf, gain, id_row = call(
        fetch_columns_body,
        (
            shaped((4 * columns, width), BF16), shaped((heads, width), BF16),
            shaped((heads, width), BF16), shaped((1, width)), shaped((1, LANES)),
        ),
        [SMEM_SPEC] * 2 + [HBM_SPEC] * 7,
        [pltpu.SemaphoreType.DMA((7,))],
        limit=4 * MIB,
    )(
        *ids, in_hbm(query_weight.T), in_hbm(key_weight.T), in_hbm(value_weight.T),
        in_hbm(outgate_weight.T), in_hbm(input_weight.T), in_hbm(forget_weight.T),
        in_hbm(mixer_gain[None]),
    )
    cols, pre = call(
        columns_body,
        (shaped((devices, 4 * columns + LANES), BF16), shaped((2 * heads, devices))),
        [VMEM_SPEC] * 6,
    )(rows, id_row, gain, stacked, wi, wf)
    parts = exchange(cols)

    memory = memory_matrix.reshape(heads, head_dim, head_dim)
    tiles = width // LANES
    early = heads // 2
    early_memory, norm, most, bias = call(
        fetch_cell_body,
        (
            shaped((early, head_dim, head_dim)), shaped((heads, head_dim)),
            shaped((1, heads)), shaped((1, heads)),
        ),
        [HBM_SPEC] * 4,
        [pltpu.SemaphoreType.DMA((4,))],
        limit=24 * MIB,
    )(in_hbm(lax.optimization_barrier((memory, pre))[0]), in_hbm(memory_norm.reshape(heads, head_dim)), in_hbm(memory_max), in_hbm(forget_bias[None]))
    gated, next_norm, next_max, value, key, keep = call(
        cell_body,
        (
            shaped((devices, width), BF16), shaped((heads, head_dim)), shaped((1, heads)),
            shaped((heads, head_dim)), shaped((heads, head_dim)), shaped((heads, head_dim)),
        ),
        [SMEM_SPEC] + [VMEM_SPEC] * 6 + [HBM_SPEC],
        [
            pltpu.VMEM((heads - early, head_dim, head_dim), F32),
            pltpu.VMEM((pl.cdiv(4 * columns, LANES), devices, LANES), F32),
            pltpu.VMEM((4 * tiles, LANES), F32),
            pltpu.SemaphoreType.DMA((heads - early,)),
        ],
        limit=24 * MIB,
    )(me[None], parts, pre, most, bias, norm, early_memory, in_hbm(memory))
    gated_rows = exchange(gated)
    next_matrix = keep[:, :, None] * memory + value[:, :, None] * key[:, None, :]

    take, mine, spread, weights = call(
        tables_body,
        (
            shaped((CAPACITY + 1, devices, devices), BF16), shaped((SLOTS, devices), BF16),
            shaped((devices, SLOTS), BF16), shaped((devices, 1)),
        ),
        [SMEM_SPEC] * 5 + [VMEM_SPEC],
    )(me[None], *ids, group_weight, member_weight.reshape(-1), parts)

    outgoing = call(
        project_body, shaped((devices, (CAPACITY + 1) * columns), BF16), [VMEM_SPEC] * 3
    )(gated_rows, mixer_out.T, take)
    incoming = exchange(outgoing)

    back, middle = call(
        expert_body,
        (shaped((devices, width), BF16), shaped((1, width))),
        [VMEM_SPEC] * 5 + [HBM_SPEC] * 3,
        [
            pltpu.VMEM((width, hidden_dim), BF16),
            pltpu.VMEM((width, hidden_dim), BF16),
            pltpu.VMEM((hidden_dim, width), BF16),
            pltpu.VMEM((pl.cdiv((CAPACITY + 1) * columns, LANES), devices, LANES), F32),
            pltpu.VMEM((SLOTS * tiles, LANES), F32),
            pltpu.SemaphoreType.DMA((3, 4)),
        ],
        limit=24 * MIB,
    )(
        incoming, rows, mine, spread, expert_gain[None],
        in_hbm(expert_gate.reshape(width, hidden_dim)), in_hbm(expert_up.reshape(width, hidden_dim)),
        in_hbm(expert_down.reshape(hidden_dim, width)),
    )
    returned = exchange(back)
    layer_out = call(finish_body, shaped((1, width), BF16), [VMEM_SPEC] * 3)(returned, weights, middle)
    return (layer_out, next_matrix[None], next_norm[None], next_max)


def solution(mesh):
    placed = (
        P("ep", None),
        P(),
        P(None, "ep"),
        P(None, "ep"),
        P(None, "ep"),
        P(None, "ep"),
        P(),
        P(),
        P(),
        P("ep", None, None, None),
        P("ep", None, None),
        P("ep", None),
        P(None, "ep"),
        P(),
        P("ep", None, None),
        P("ep", None, None),
        P("ep", None, None),
        P("ep"),
        P("ep", None),
        P("ep"),
        P("ep", None),
    )
    return jax.shard_map(
        local,
        mesh=mesh,
        in_specs=placed,
        out_specs=(P("ep", None), P("ep", None, None, None), P("ep", None, None), P("ep", None)),
        check_vma=False,
    )
```

```python
import jax
import jax.numpy as jnp
from jax import lax
from jax.experimental import pallas as pl
from jax.experimental.pallas import tpu as pltpu
from jax.sharding import PartitionSpec as P

GROUPS = 4
CAPACITY = 4
LANES = 128
SLOTS = 8
MIB = 1 << 20
AHEAD = 2_000_000_000
F32 = jnp.float32
BF16 = jnp.bfloat16
NT = (((1,), (1,)), ((), ()))


norm_eps = 1e-06


def root_norm(values, gain):
    return values * lax.rsqrt(jnp.mean(values * values, axis=-1, keepdims=True) + norm_eps) * gain


def exchange(blocks):
    count, width = blocks.shape
    halves = blocks.reshape(count, 2, width // 2)
    return lax.all_to_all(halves, "ep", split_axis=0, concat_axis=0, tiled=True).reshape(count, width)


VMEM_SPEC = pl.BlockSpec(memory_space=pltpu.VMEM)
SMEM_SPEC = pl.BlockSpec(memory_space=pltpu.SMEM)
HBM_SPEC = pl.BlockSpec(memory_space=pltpu.HBM)


def call(body, outs, ins, scratch=(), limit=8 * MIB, flops=10_000_000, moved=1_000_000):
    return pl.pallas_call(
        body,
        out_shape=outs,
        in_specs=ins,
        out_specs=jax.tree.map(lambda _: VMEM_SPEC, outs),
        scratch_shapes=scratch,
        compiler_params=pltpu.CompilerParams(vmem_limit_bytes=limit),
        cost_estimate=pl.CostEstimate(flops=flops, bytes_accessed=moved, transcendentals=0),
    )


def in_hbm(array):
    return pltpu.with_memory_space_constraint(array, pltpu.HBM)


def shaped(shape, dtype=F32):
    return jax.ShapeDtypeStruct(shape, dtype)


def feature_rows(ref, offset, columns):
    group = LANES // columns
    count = ref.shape[1] // group
    tile, lane = divmod(offset, LANES)
    pieces = [
        ref[tile, pl.ds(g, count, stride=group), :][:, lane:lane + columns] for g in range(group)
    ]
    return jnp.concatenate(pieces, axis=1)


def spill(ref, values):
    for t in range(ref.shape[0]):
        part = values[:, t * LANES:(t + 1) * LANES]
        ref[t, :, :part.shape[1]] = part


def diagonal(n):
    i = lax.broadcasted_iota(jnp.int32, (n, n), 0)
    j = lax.broadcasted_iota(jnp.int32, (n, n), 1)
    return i == j


def to_column(row):
    n = row.shape[1]
    spread = jnp.broadcast_to(row, (n, n))
    return jnp.sum(jnp.where(diagonal(n), spread, 0.0), axis=1, keepdims=True)


def to_row(col):
    n = col.shape[0]
    spread = jnp.broadcast_to(col, (n, n))
    return jnp.sum(jnp.where(diagonal(n), spread, 0.0), axis=0, keepdims=True)


def spread_body(me_ref, group_ref, weight_ref, row_ref, out_ref):
    del me_ref, group_ref, weight_ref
    out_ref[...] = jnp.broadcast_to(row_ref[...].astype(F32), out_ref.shape).astype(BF16)


def columns_body(group_ref, member_ref, rows_ref, gain_ref, wq, wk, wv, wo, wi, wf, out_ref, pre_ref):
    heads = wi.shape[0]
    count = rows_ref.shape[0]
    normed = root_norm(rows_ref[...].astype(F32), gain_ref[...]).astype(BF16)
    cols = [
        lax.dot_general(normed, w[...], NT, preferred_element_type=F32) for w in (wq, wk, wv, wo)
    ]
    cols = jnp.concatenate(cols, axis=1).astype(BF16)
    total = cols.shape[1]
    out_ref[:, :total] = cols
    lane = lax.broadcasted_iota(jnp.int32, (count, out_ref.shape[1] - total), 1)
    ids = jnp.where(lane == 0, group_ref[0], 0)
    for k in range(member_ref.shape[0]):
        ids = jnp.where(lane == 1 + k, member_ref[k], ids)
    out_ref[:, total:] = ids.astype(F32).astype(BF16)
    pre_ref[:heads, :] = lax.dot_general(wi[...], normed, NT, preferred_element_type=F32)
    pre_ref[heads:, :] = lax.dot_general(wf[...], normed, NT, preferred_element_type=F32)


def tables_body(
    me_ref, group_ref, member_ref, group_weight, member_weight, parts_ref, norm_ref, max_ref, gate_ref,
    take_ref, mine_ref, spread_ref, weight_ref, norm_out, max_out, early_ref,
    sem,
):
    fetch = pltpu.make_async_copy(gate_ref.at[pl.ds(0, early_ref.shape[0])], early_ref, sem)
    fetch.start()
    norm_out[...] = norm_ref[...]
    max_out[...] = max_ref[...]

    count = parts_ref.shape[0]
    members = count // GROUPS
    picks = member_ref.shape[0]
    ids = parts_ref[:, parts_ref.shape[1] - LANES:].astype(F32)
    lane = lax.broadcasted_iota(jnp.int32, ids.shape, 1)

    def row_of(k):
        return to_row(jnp.sum(jnp.where(lane == k, ids, 0.0), axis=1, keepdims=True))

    group = row_of(0)
    expert = lax.broadcasted_iota(jnp.int32, (count, count), 0)
    token = lax.broadcasted_iota(jnp.int32, (count, count), 1)
    hit = jnp.zeros((count, count), F32)
    column = lax.broadcasted_iota(jnp.int32, (count, 1), 0)
    weight = jnp.zeros((count, 1), F32)
    for k in range(picks):
        chosen = (group * members + row_of(1 + k)).astype(jnp.int32)
        hit = jnp.where(expert == chosen, 1.0, hit)
        local = group_ref[0] * members + member_ref[k]
        weight += jnp.where(column == local, group_weight[0] * member_weight[k], 0.0)
    weight_ref[...] = weight
    upto = jnp.where(expert <= token, 1.0, 0.0).astype(BF16)
    place = jnp.dot(hit.astype(BF16), upto, preferred_element_type=F32)
    slot = lax.broadcasted_iota(jnp.int32, (SLOTS, count), 0)
    lane = lax.broadcasted_iota(jnp.int32, (count, SLOTS), 1)
    mine = jnp.zeros((SLOTS, count), F32)
    spread = jnp.zeros((count, SLOTS), F32)
    for s in range(CAPACITY + 1):
        if s < CAPACITY:
            take = jnp.where(place == s + 1.0, hit, 0.0)
        else:
            take = jnp.where(expert == token, 1.0, 0.0)
        take_ref[s] = take.astype(BF16)
        row = jnp.sum(jnp.where(expert == me_ref[0], take, 0.0), axis=0, keepdims=True)
        mine = jnp.where(slot == s, row, mine)
        if s < CAPACITY:
            spread = jnp.where(lane == s, to_column(row), spread)
    mine_ref[...] = mine.astype(BF16)
    spread_ref[...] = spread.astype(BF16)
    fetch.wait()


def cell_body(
    me_ref, parts_ref, pre_ref, max_ref, bias_ref, norm_ref, mem_ref,
    gated_ref, norm_out, max_out, value_out, key_out, keep_out,
    mem, wide, tall, sems,
):
    heads, head_dim = norm_ref.shape
    copies = [pltpu.make_async_copy(mem_ref.at[h], mem.at[h], sems.at[h]) for h in range(heads)]
    for c in copies:
        c.start()

    columns = (parts_ref.shape[1] - LANES) // 4
    tiles = head_dim // LANES
    rows = heads * tiles
    spill(wide, parts_ref[:, :4 * columns].astype(F32))
    for n in range(4):
        tall[n * rows:(n + 1) * rows, :] = feature_rows(wide, n * columns, columns)

    def heads_of(n):
        return jnp.concatenate(
            [tall[pl.ds(n * rows + p, heads, stride=tiles), :] for p in range(tiles)], axis=1
        )

    query, key, value, outgate = (heads_of(n) for n in range(4))
    key = key * head_dim ** (-0.5)

    pre = pre_ref[...]
    lane = lax.broadcasted_iota(jnp.int32, pre.shape, 1)
    pre = jnp.sum(jnp.where(lane == me_ref[0], pre, 0.0), axis=1, keepdims=True)
    input_pre = pre[:heads]
    forget_pre = pre[heads:] + to_column(bias_ref[...])
    log_forget = jnp.minimum(forget_pre, 0.0) - jnp.log1p(jnp.exp(-jnp.abs(forget_pre)))
    carry = log_forget + to_column(max_ref[...])
    next_max = jnp.maximum(carry, input_pre)
    keep = jnp.exp(carry - next_max)
    admit = jnp.exp(input_pre - next_max)

    norm = norm_ref[...]
    score = admit * jnp.sum(key * query, axis=1, keepdims=True)
    denom = keep * jnp.sum(norm * query, axis=1, keepdims=True) + score
    scale = 1.0 / jnp.maximum(jnp.abs(denom), jnp.exp(-next_max))
    opened = jax.nn.sigmoid(outgate)
    norm_out[...] = keep * norm + admit * key
    max_out[...] = to_row(next_max)
    value_out[...] = admit * value
    key_out[...] = key
    keep_out[...] = jnp.broadcast_to(keep, keep_out.shape)

    count = gated_ref.shape[0]
    left = jnp.concatenate([query, jnp.zeros((8 - heads, head_dim), F32)], axis=0) if heads < 8 else query
    left = left.astype(BF16)
    for h in range(heads):
        copies[h].wait()
        block = mem[h]
        high = block.astype(BF16)
        low = (block - high.astype(F32)).astype(BF16)
        carried = lax.dot_general(left, high, NT, preferred_element_type=F32)
        carried = carried + lax.dot_general(left, low, NT, preferred_element_type=F32)
        carried = carried[h:h + 1]
        numer = keep[h:h + 1] * carried + score[h:h + 1] * value[h:h + 1]
        gated = numer * scale[h:h + 1] * opened[h:h + 1]
        gated_ref[:, h * head_dim:(h + 1) * head_dim] = jnp.broadcast_to(
            gated, (count, head_dim)
        ).astype(BF16)


def project_body(gated_ref, weight_ref, take_ref, done_ref, out_ref):
    del done_ref
    proj = lax.dot_general(gated_ref[...], weight_ref[...], NT, preferred_element_type=F32).astype(BF16)
    blocks = [
        jnp.dot(take_ref[s], proj, preferred_element_type=F32) for s in range(take_ref.shape[0])
    ]
    out_ref[...] = jnp.concatenate(blocks, axis=1).astype(BF16)


def expert_body(
    in_ref, rows_ref, mine_ref, spread_ref, gain_ref, early_ref, gate_ref, up_ref, down_ref,
    out_ref, middle_ref,
    gate, up, down, wide, tall, sems,
):
    width, hidden_dim = gate_ref.shape
    steps = sems.shape[1]
    here = early_ref.shape[0] * steps // width
    wide_step = width // steps
    tall_step = hidden_dim // steps

    def chunk(n, src, dst, k, step, skip=0):
        return pltpu.make_async_copy(
            src.at[pl.ds(k * step, step)], dst.at[pl.ds(k * step - skip, step)], sems.at[n, k]
        )

    gates = [None] * here + [
        chunk(0, gate_ref, gate, k, wide_step, early_ref.shape[0]) for k in range(here, steps)
    ]
    ups = [chunk(1, up_ref, up, k, wide_step) for k in range(steps)]
    downs = [chunk(2, down_ref, down, k, tall_step) for k in range(steps)]
    for k in range(steps):
        ups[k].start()
        if k >= here:
            gates[k].start()
    for k in range(steps):
        downs[k].start()

    used = CAPACITY + 1
    columns = in_ref.shape[1] // used
    tiles = width // LANES
    spill(wide, in_ref[...].astype(F32))
    for s in range(used):
        tall[s * tiles:(s + 1) * tiles, :] = feature_rows(wide, s * columns, columns)
    tall[used * tiles:, :] = jnp.zeros((tall.shape[0] - used * tiles, LANES), F32)
    projected = jnp.concatenate(
        [tall[pl.ds(r, SLOTS, stride=tiles), :] for r in range(tiles)], axis=1
    )
    resid = jnp.dot(mine_ref[...], rows_ref[...], preferred_element_type=F32)
    middle = (resid + projected).astype(BF16).astype(F32)
    middle_ref[...] = middle[CAPACITY:CAPACITY + 1]
    left = root_norm(middle, gain_ref[...]).astype(BF16)

    gate_part = jnp.dot(left[:, :here * wide_step], early_ref[...], preferred_element_type=F32)
    up_part = jnp.zeros((SLOTS, hidden_dim), F32)
    for k in range(steps):
        part = slice(k * wide_step, (k + 1) * wide_step)
        ups[k].wait()
        up_part += jnp.dot(left[:, part], up[part, :], preferred_element_type=F32)
        if k >= here:
            gates[k].wait()
            block = gate[(k - here) * wide_step:(k - here + 1) * wide_step, :]
            gate_part += jnp.dot(left[:, part], block, preferred_element_type=F32)
    hidden = (gate_part / (1.0 + jnp.exp(-gate_part)) * up_part).astype(BF16)
    result = jnp.zeros((SLOTS, width), F32)
    for k in range(steps):
        part = slice(k * tall_step, (k + 1) * tall_step)
        downs[k].wait()
        result += jnp.dot(hidden[:, part], down[part, :], preferred_element_type=F32)
    out_ref[...] = jnp.dot(
        spread_ref[...], result.astype(BF16), preferred_element_type=F32
    ).astype(BF16)


def finish_body(returned_ref, weight_ref, middle_ref, out_ref):
    mixture = jnp.sum(weight_ref[...] * returned_ref[...].astype(F32), axis=0, keepdims=True)
    out_ref[...] = (middle_ref[...] + mixture).astype(BF16)


def local(
    tokens,
    mixer_gain,
    query_weight,
    key_weight,
    value_weight,
    outgate_weight,
    input_weight,
    forget_weight,
    forget_bias,
    memory_matrix,
    memory_norm,
    memory_max,
    mixer_out,
    expert_gain,
    expert_gate,
    expert_up,
    expert_down,
    route_group,
    route_member,
    group_weight,
    member_weight,
):
    devices = lax.axis_size("ep")
    width = tokens.shape[1]
    columns = query_weight.shape[1]
    heads, head_dim = memory_norm.shape[1:]
    hidden_dim = expert_gate.shape[2]
    assert tokens.shape[0] == 1 and expert_gate.shape[0] == 1
    me = lax.axis_index("ep").astype(jnp.int32)[None]

    ids = (route_group, route_member.reshape(-1))

    row = call(spread_body, shaped((devices, width), BF16), [SMEM_SPEC] * 3 + [VMEM_SPEC], flops=AHEAD)(
        me, route_group, group_weight, tokens
    )
    rows = exchange(row)

    cols, pre = call(
        columns_body,
        (shaped((devices, 4 * columns + LANES), BF16), shaped((2 * heads, devices))),
        [SMEM_SPEC] * 2 + [VMEM_SPEC] * 8,
        flops=AHEAD,
    )(
        *ids, rows, mixer_gain[None], query_weight.T, key_weight.T, value_weight.T, outgate_weight.T,
        input_weight.T, forget_weight.T,
    )
    parts = exchange(cols)

    memory = memory_matrix.reshape(heads, head_dim, head_dim)
    tiles = width // LANES
    gated, next_norm, next_max, value, key, keep = call(
        cell_body,
        (
            shaped((devices, width), BF16), shaped((heads, head_dim)), shaped((1, heads)),
            shaped((heads, head_dim)), shaped((heads, head_dim)), shaped((heads, head_dim)),
        ),
        [SMEM_SPEC] + [VMEM_SPEC] * 5 + [HBM_SPEC],
        [
            pltpu.VMEM((heads, head_dim, head_dim), F32),
            pltpu.VMEM((pl.cdiv(4 * columns, LANES), devices, LANES), F32),
            pltpu.VMEM((4 * tiles, LANES), F32),
            pltpu.SemaphoreType.DMA((heads,)),
        ],
        limit=12 * MIB,
        flops=AHEAD,
    )(
        me, parts, pre, memory_max, forget_bias[None], memory_norm.reshape(heads, head_dim),
        in_hbm(memory),
    )
    gated_rows = exchange(gated)

    next_matrix = keep[:, :, None] * memory + value[:, :, None] * key[:, None, :]
    next_matrix = lax.optimization_barrier(next_matrix[None])
    gate = in_hbm(expert_gate.reshape(width, hidden_dim))
    take, mine, spread, weights, next_norm, next_max, early = call(
        tables_body,
        (
            shaped((CAPACITY + 1, devices, devices), BF16), shaped((SLOTS, devices), BF16),
            shaped((devices, SLOTS), BF16), shaped((devices, 1)),
            shaped((heads, head_dim)), shaped((1, heads)), shaped((width // 2, hidden_dim), BF16),
        ),
        [SMEM_SPEC] * 5 + [VMEM_SPEC] * 3 + [HBM_SPEC],
        [pltpu.SemaphoreType.DMA],
    )(me, *ids, group_weight, member_weight.reshape(-1), parts, next_norm, next_max, gate)

    outgoing = call(
        project_body, shaped((devices, (CAPACITY + 1) * columns), BF16), [VMEM_SPEC] * 3 + [HBM_SPEC],
    )(gated_rows, mixer_out.T, take, in_hbm(next_matrix))
    incoming = exchange(outgoing)

    back, middle = call(
        expert_body,
        (shaped((devices, width), BF16), shaped((1, width))),
        [VMEM_SPEC] * 6 + [HBM_SPEC] * 3,
        [
            pltpu.VMEM((width - width // 2, hidden_dim), BF16),
            pltpu.VMEM((width, hidden_dim), BF16),
            pltpu.VMEM((hidden_dim, width), BF16),
            pltpu.VMEM((pl.cdiv((CAPACITY + 1) * columns, LANES), devices, LANES), F32),
            pltpu.VMEM((SLOTS * tiles, LANES), F32),
            pltpu.SemaphoreType.DMA((3, 4)),
        ],
        limit=24 * MIB,
    )(
        incoming, rows, mine, spread, expert_gain[None], early, gate,
        in_hbm(expert_up.reshape(width, hidden_dim)),
        in_hbm(expert_down.reshape(hidden_dim, width)),
    )
    returned = exchange(back)
    layer_out = call(finish_body, shaped((1, width), BF16), [VMEM_SPEC] * 3)(returned, weights, middle)
    return (layer_out, next_matrix, next_norm[None], next_max)


def solution(mesh):
    placed = (
        P("ep", None),
        P(),
        P(None, "ep"),
        P(None, "ep"),
        P(None, "ep"),
        P(None, "ep"),
        P(),
        P(),
        P(),
        P("ep", None, None, None),
        P("ep", None, None),
        P("ep", None),
        P(None, "ep"),
        P(),
        P("ep", None, None),
        P("ep", None, None),
        P("ep", None, None),
        P("ep"),
        P("ep", None),
        P("ep"),
        P("ep", None),
    )
    return jax.shard_map(
        local,
        mesh=mesh,
        in_specs=placed,
        out_specs=(P("ep", None), P("ep", None, None, None), P("ep", None, None), P("ep", None)),
        check_vma=False,
    )
```

```python
import jax
import jax.numpy as jnp
from jax import lax
from jax.experimental import pallas as pl
from jax.experimental.pallas import tpu as pltpu
from jax.sharding import PartitionSpec as P

GROUPS = 4
CAPACITY = 4
LANES = 128
SLOTS = 8
MIB = 1 << 20
AHEAD = 2_000_000_000
F32 = jnp.float32
BF16 = jnp.bfloat16
NT = (((1,), (1,)), ((), ()))


norm_eps = 1e-06


def root_norm(values, gain):
    return values * lax.rsqrt(jnp.mean(values * values, axis=-1, keepdims=True) + norm_eps) * gain


def exchange(blocks):
    count, width = blocks.shape
    halves = blocks.reshape(count, 2, width // 2)
    return lax.all_to_all(halves, "ep", split_axis=0, concat_axis=0, tiled=True).reshape(count, width)


VMEM_SPEC = pl.BlockSpec(memory_space=pltpu.VMEM)
SMEM_SPEC = pl.BlockSpec(memory_space=pltpu.SMEM)
HBM_SPEC = pl.BlockSpec(memory_space=pltpu.HBM)


def call(body, outs, ins, scratch=(), outputs=None, aliases={}, limit=8 * MIB, flops=10_000_000, moved=1_000_000):
    return pl.pallas_call(
        body,
        out_shape=outs,
        in_specs=ins,
        out_specs=outputs or jax.tree.map(lambda _: VMEM_SPEC, outs),
        scratch_shapes=scratch,
        input_output_aliases=aliases,
        compiler_params=pltpu.CompilerParams(vmem_limit_bytes=limit),
        cost_estimate=pl.CostEstimate(flops=flops, bytes_accessed=moved, transcendentals=0),
    )


def in_hbm(array):
    return pltpu.with_memory_space_constraint(array, pltpu.HBM)


def shaped(shape, dtype=F32):
    return jax.ShapeDtypeStruct(shape, dtype)


def feature_rows(ref, offset, columns):
    group = LANES // columns
    count = ref.shape[1] // group
    tile, lane = divmod(offset, LANES)
    pieces = [
        ref[tile, pl.ds(g, count, stride=group), :][:, lane:lane + columns] for g in range(group)
    ]
    return jnp.concatenate(pieces, axis=1)


def spill(ref, values):
    for t in range(ref.shape[0]):
        part = values[:, t * LANES:(t + 1) * LANES]
        ref[t, :, :part.shape[1]] = part


def diagonal(n):
    i = lax.broadcasted_iota(jnp.int32, (n, n), 0)
    j = lax.broadcasted_iota(jnp.int32, (n, n), 1)
    return i == j


def to_column(row):
    n = row.shape[1]
    spread = jnp.broadcast_to(row, (n, n))
    return jnp.sum(jnp.where(diagonal(n), spread, 0.0), axis=1, keepdims=True)


def to_row(col):
    n = col.shape[0]
    spread = jnp.broadcast_to(col, (n, n))
    return jnp.sum(jnp.where(diagonal(n), spread, 0.0), axis=0, keepdims=True)


def spread_body(me_ref, group_ref, weight_ref, row_ref, out_ref):
    del me_ref, group_ref, weight_ref
    out_ref[...] = jnp.broadcast_to(row_ref[...].astype(F32), out_ref.shape).astype(BF16)


def columns_body(group_ref, member_ref, rows_ref, gain_ref, wq, wk, wv, wo, wi, wf, out_ref, pre_ref):
    heads = wi.shape[0]
    count = rows_ref.shape[0]
    normed = root_norm(rows_ref[...].astype(F32), gain_ref[...]).astype(BF16)
    stacked = jnp.concatenate([w[...] for w in (wq, wk, wv, wo)], axis=0)
    cols = lax.dot_general(normed, stacked, NT, preferred_element_type=F32).astype(BF16)
    total = cols.shape[1]
    out_ref[:, :total] = cols
    lane = lax.broadcasted_iota(jnp.int32, (count, out_ref.shape[1] - total), 1)
    ids = jnp.where(lane == 0, group_ref[0], 0)
    for k in range(member_ref.shape[0]):
        ids = jnp.where(lane == 1 + k, member_ref[k], ids)
    out_ref[:, total:] = ids.astype(F32).astype(BF16)
    pre_ref[:heads, :] = lax.dot_general(wi[...], normed, NT, preferred_element_type=F32)
    pre_ref[heads:, :] = lax.dot_general(wf[...], normed, NT, preferred_element_type=F32)


def window_body(
    me_ref, group_ref, member_ref, group_weight, member_weight, parts_ref, norm_ref, max_ref,
    value_ref, key_ref, keep_ref, mem_ref, gate_ref, begun_ref,
    take_ref, mine_ref, spread_ref, weight_ref, norm_out, max_out, early_ref, next_ref,
    old, new, sems,
):
    del begun_ref
    late = old.shape[0]
    first = next_ref.shape[0] - late
    loads = [
        pltpu.make_async_copy(mem_ref.at[first + h], old.at[h], sems.at[0, h]) for h in range(late)
    ]
    stores = [
        pltpu.make_async_copy(new.at[h], next_ref.at[first + h], sems.at[1, h]) for h in range(late)
    ]
    fetch = pltpu.make_async_copy(gate_ref.at[pl.ds(0, early_ref.shape[0])], early_ref, sems.at[0, late])
    for c in loads:
        c.start()
    fetch.start()
    norm_out[...] = norm_ref[...]
    max_out[...] = max_ref[...]
    slot_tables(
        me_ref, group_ref, member_ref, group_weight, member_weight, parts_ref,
        take_ref, mine_ref, spread_ref, weight_ref,
    )
    turned = columns_of(value_ref[...])
    for h in range(late):
        row = slice(first + h, first + h + 1)
        loads[h].wait()
        new[h] = keep_ref[row] * old[h] + turned[:, row] * key_ref[row]
        stores[h].start()
    fetch.wait()
    for c in stores:
        c.wait()


def slot_tables(
    me_ref, group_ref, member_ref, group_weight, member_weight, parts_ref,
    take_ref, mine_ref, spread_ref, weight_ref,
):
    count = parts_ref.shape[0]
    members = count // GROUPS
    picks = member_ref.shape[0]
    ids = parts_ref[:, parts_ref.shape[1] - LANES:].astype(F32)
    lane = lax.broadcasted_iota(jnp.int32, ids.shape, 1)

    def row_of(k):
        return to_row(jnp.sum(jnp.where(lane == k, ids, 0.0), axis=1, keepdims=True))

    group = row_of(0)
    expert = lax.broadcasted_iota(jnp.int32, (count, count), 0)
    token = lax.broadcasted_iota(jnp.int32, (count, count), 1)
    hit = jnp.zeros((count, count), F32)
    column = lax.broadcasted_iota(jnp.int32, (count, 1), 0)
    weight = jnp.zeros((count, 1), F32)
    for k in range(picks):
        chosen = (group * members + row_of(1 + k)).astype(jnp.int32)
        hit = jnp.where(expert == chosen, 1.0, hit)
        local = group_ref[0] * members + member_ref[k]
        weight += jnp.where(column == local, group_weight[0] * member_weight[k], 0.0)
    weight_ref[...] = weight
    upto = jnp.where(expert <= token, 1.0, 0.0).astype(BF16)
    place = jnp.dot(hit.astype(BF16), upto, preferred_element_type=F32)
    slot = lax.broadcasted_iota(jnp.int32, (SLOTS, count), 0)
    lane = lax.broadcasted_iota(jnp.int32, (count, SLOTS), 1)
    mine = jnp.zeros((SLOTS, count), F32)
    spread = jnp.zeros((count, SLOTS), F32)
    for s in range(CAPACITY + 1):
        if s < CAPACITY:
            take = jnp.where(place == s + 1.0, hit, 0.0)
        else:
            take = jnp.where(expert == token, 1.0, 0.0)
        take_ref[s] = take.astype(BF16)
        row = jnp.sum(jnp.where(expert == me_ref[0], take, 0.0), axis=0, keepdims=True)
        mine = jnp.where(slot == s, row, mine)
        if s < CAPACITY:
            spread = jnp.where(lane == s, to_column(row), spread)
    mine_ref[...] = mine.astype(BF16)
    spread_ref[...] = spread.astype(BF16)


def cell_body(
    me_ref, parts_ref, pre_ref, max_ref, bias_ref, norm_ref, mem_ref,
    gated_ref, norm_out, max_out, value_out, key_out, keep_out, next_ref,
    mem, new, wide, tall, sems,
):
    heads, head_dim = norm_ref.shape
    first = new.shape[0]
    copies = [pltpu.make_async_copy(mem_ref.at[h], mem.at[h], sems.at[0, h]) for h in range(heads)]
    stores = [pltpu.make_async_copy(new.at[h], next_ref.at[h], sems.at[1, h]) for h in range(first)]
    for c in copies:
        c.start()

    columns = (parts_ref.shape[1] - LANES) // 4
    tiles = head_dim // LANES
    rows = heads * tiles
    spill(wide, parts_ref[:, :4 * columns].astype(F32))
    for n in range(4):
        tall[n * rows:(n + 1) * rows, :] = feature_rows(wide, n * columns, columns)

    def heads_of(n):
        return jnp.concatenate(
            [tall[pl.ds(n * rows + p, heads, stride=tiles), :] for p in range(tiles)], axis=1
        )

    query, key, value, outgate = (heads_of(n) for n in range(4))
    key = key * head_dim ** (-0.5)

    pre = pre_ref[...]
    lane = lax.broadcasted_iota(jnp.int32, pre.shape, 1)
    pre = jnp.sum(jnp.where(lane == me_ref[0], pre, 0.0), axis=1, keepdims=True)
    input_pre = pre[:heads]
    forget_pre = pre[heads:] + to_column(bias_ref[...])
    log_forget = jnp.minimum(forget_pre, 0.0) - jnp.log1p(jnp.exp(-jnp.abs(forget_pre)))
    carry = log_forget + to_column(max_ref[...])
    next_max = jnp.maximum(carry, input_pre)
    keep = jnp.exp(carry - next_max)
    admit = jnp.exp(input_pre - next_max)

    norm = norm_ref[...]
    score = admit * jnp.sum(key * query, axis=1, keepdims=True)
    denom = keep * jnp.sum(norm * query, axis=1, keepdims=True) + score
    scale = 1.0 / jnp.maximum(jnp.abs(denom), jnp.exp(-next_max))
    opened = jax.nn.sigmoid(outgate)
    norm_out[...] = keep * norm + admit * key
    max_out[...] = to_row(next_max)
    value_out[...] = admit * value
    key_out[...] = key
    keep_out[...] = jnp.broadcast_to(keep, keep_out.shape)

    count = gated_ref.shape[0]
    ones = jnp.ones((8, LANES), BF16)
    turned = columns_of(admit * value)
    for h in range(heads):
        copies[h].wait()
        sums = []
        for r in range(0, head_dim, LANES):
            block = mem[h, r:r + LANES, :]
            product = block * query[h:h + 1]
            sums.append(sum(product[:, p * LANES:(p + 1) * LANES] for p in range(tiles)))
            if h < first:
                new[h, r:r + LANES, :] = (
                    keep[h:h + 1] * block + turned[r:r + LANES, h:h + 1] * key[h:h + 1]
                )
        if h < first:
            stores[h].start()
        sums = jnp.concatenate(sums, axis=0)
        high = sums.astype(BF16)
        low = (sums - high.astype(F32)).astype(BF16)
        carried = lax.dot_general(ones, high, NT, preferred_element_type=F32)
        carried = carried + lax.dot_general(ones, low, NT, preferred_element_type=F32)
        numer = keep[h:h + 1] * carried[:1] + score[h:h + 1] * value[h:h + 1]
        gated = numer * scale[h:h + 1] * opened[h:h + 1]
        gated_ref[:, h * head_dim:(h + 1) * head_dim] = jnp.broadcast_to(
            gated, (count, head_dim)
        ).astype(BF16)
    for c in stores:
        c.wait()


def columns_of(value):
    heads = value.shape[0]
    if heads < 8:
        value = jnp.concatenate([value, jnp.zeros((8 - heads, value.shape[1]), F32)], axis=0)
    return value.T


def project_body(gated_ref, weight_ref, take_ref, out_ref):
    proj = lax.dot_general(gated_ref[...], weight_ref[...], NT, preferred_element_type=F32).astype(BF16)
    blocks = [
        jnp.dot(take_ref[s], proj, preferred_element_type=F32) for s in range(take_ref.shape[0])
    ]
    out_ref[...] = jnp.concatenate(blocks, axis=1).astype(BF16)


def expert_body(
    in_ref, rows_ref, mine_ref, spread_ref, gain_ref, early_ref, gate_ref, up_ref, down_ref,
    out_ref, middle_ref,
    gate, up, down, wide, tall, sems,
):
    width, hidden_dim = gate_ref.shape
    steps = sems.shape[1]
    here = early_ref.shape[0] * steps // width
    wide_step = width // steps
    tall_step = hidden_dim // steps

    def chunk(n, src, dst, k, step, skip=0):
        return pltpu.make_async_copy(
            src.at[pl.ds(k * step, step)], dst.at[pl.ds(k * step - skip, step)], sems.at[n, k]
        )

    gates = [None] * here + [
        chunk(0, gate_ref, gate, k, wide_step, early_ref.shape[0]) for k in range(here, steps)
    ]
    ups = [chunk(1, up_ref, up, k, wide_step) for k in range(steps)]
    downs = [chunk(2, down_ref, down, k, tall_step) for k in range(steps)]
    for k in range(steps):
        ups[k].start()
        if k >= here:
            gates[k].start()
    for k in range(steps):
        downs[k].start()

    used = CAPACITY + 1
    columns = in_ref.shape[1] // used
    tiles = width // LANES
    spill(wide, in_ref[...].astype(F32))
    for s in range(used):
        tall[s * tiles:(s + 1) * tiles, :] = feature_rows(wide, s * columns, columns)
    tall[used * tiles:, :] = jnp.zeros((tall.shape[0] - used * tiles, LANES), F32)
    projected = jnp.concatenate(
        [tall[pl.ds(r, SLOTS, stride=tiles), :] for r in range(tiles)], axis=1
    )
    resid = jnp.dot(mine_ref[...], rows_ref[...], preferred_element_type=F32)
    middle = (resid + projected).astype(BF16).astype(F32)
    middle_ref[...] = middle[CAPACITY:CAPACITY + 1]
    left = root_norm(middle, gain_ref[...]).astype(BF16)

    gate_part = jnp.dot(left[:, :here * wide_step], early_ref[...], preferred_element_type=F32)
    up_part = jnp.zeros((SLOTS, hidden_dim), F32)
    for k in range(steps):
        part = slice(k * wide_step, (k + 1) * wide_step)
        ups[k].wait()
        up_part += jnp.dot(left[:, part], up[part, :], preferred_element_type=F32)
        if k >= here:
            gates[k].wait()
            block = gate[(k - here) * wide_step:(k - here + 1) * wide_step, :]
            gate_part += jnp.dot(left[:, part], block, preferred_element_type=F32)
    hidden = (gate_part / (1.0 + jnp.exp(-gate_part)) * up_part).astype(BF16)
    result = jnp.zeros((SLOTS, width), F32)
    for k in range(steps):
        part = slice(k * tall_step, (k + 1) * tall_step)
        downs[k].wait()
        result += jnp.dot(hidden[:, part], down[part, :], preferred_element_type=F32)
    out_ref[...] = jnp.dot(
        spread_ref[...], result.astype(BF16), preferred_element_type=F32
    ).astype(BF16)


def finish_body(returned_ref, weight_ref, middle_ref, out_ref):
    mixture = jnp.sum(weight_ref[...] * returned_ref[...].astype(F32), axis=0, keepdims=True)
    out_ref[...] = (middle_ref[...] + mixture).astype(BF16)


def local(
    tokens,
    mixer_gain,
    query_weight,
    key_weight,
    value_weight,
    outgate_weight,
    input_weight,
    forget_weight,
    forget_bias,
    memory_matrix,
    memory_norm,
    memory_max,
    mixer_out,
    expert_gain,
    expert_gate,
    expert_up,
    expert_down,
    route_group,
    route_member,
    group_weight,
    member_weight,
):
    devices = lax.axis_size("ep")
    width = tokens.shape[1]
    columns = query_weight.shape[1]
    heads, head_dim = memory_norm.shape[1:]
    hidden_dim = expert_gate.shape[2]
    assert tokens.shape[0] == 1 and expert_gate.shape[0] == 1
    me = lax.axis_index("ep").astype(jnp.int32)[None]

    ids = (route_group, route_member.reshape(-1))

    row = call(spread_body, shaped((devices, width), BF16), [SMEM_SPEC] * 3 + [VMEM_SPEC], flops=AHEAD)(
        me, route_group, group_weight, tokens
    )
    rows = exchange(row)

    cols, pre = call(
        columns_body,
        (shaped((devices, 4 * columns + LANES), BF16), shaped((2 * heads, devices))),
        [SMEM_SPEC] * 2 + [VMEM_SPEC] * 8,
        flops=AHEAD,
    )(
        *ids, rows, mixer_gain[None], query_weight.T, key_weight.T, value_weight.T, outgate_weight.T,
        input_weight.T, forget_weight.T,
    )
    parts = exchange(cols)

    memory = memory_matrix.reshape(heads, head_dim, head_dim)
    tiles = width // LANES
    first = heads // 2
    gated, next_norm, next_max, value, key, keep, begun = call(
        cell_body,
        (
            shaped((devices, width), BF16), shaped((heads, head_dim)), shaped((1, heads)),
            shaped((heads, head_dim)), shaped((heads, head_dim)), shaped((heads, head_dim)),
            shaped((heads, head_dim, head_dim)),
        ),
        [SMEM_SPEC] + [VMEM_SPEC] * 5 + [HBM_SPEC],
        [
            pltpu.VMEM((heads, head_dim, head_dim), F32),
            pltpu.VMEM((first, head_dim, head_dim), F32),
            pltpu.VMEM((pl.cdiv(4 * columns, LANES), devices, LANES), F32),
            pltpu.VMEM((4 * tiles, LANES), F32),
            pltpu.SemaphoreType.DMA((2, heads)),
        ],
        outputs=[VMEM_SPEC] * 6 + [HBM_SPEC],
        limit=16 * MIB,
        flops=AHEAD,
    )(
        me, parts, pre, memory_max, forget_bias[None], memory_norm.reshape(heads, head_dim),
        in_hbm(memory),
    )
    gated_rows = exchange(gated)

    gate = in_hbm(expert_gate.reshape(width, hidden_dim))
    early_rows = width // 2
    take, mine, spread, weights, next_norm, next_max, early, next_matrix = call(
        window_body,
        (
            shaped((CAPACITY + 1, devices, devices), BF16), shaped((SLOTS, devices), BF16),
            shaped((devices, SLOTS), BF16), shaped((devices, 1)),
            shaped((heads, head_dim)), shaped((1, heads)), shaped((early_rows, hidden_dim), BF16),
            shaped((heads, head_dim, head_dim)),
        ),
        [SMEM_SPEC] * 5 + [VMEM_SPEC] * 6 + [HBM_SPEC] * 3,
        [
            pltpu.VMEM((heads - first, head_dim, head_dim), F32),
            pltpu.VMEM((heads - first, head_dim, head_dim), F32),
            pltpu.SemaphoreType.DMA((2, heads - first + 1)),
        ],
        outputs=[VMEM_SPEC] * 7 + [HBM_SPEC],
        aliases={13: 7},
        limit=16 * MIB,
    )(
        me, *ids, group_weight, member_weight.reshape(-1), parts, next_norm, next_max,
        value, key, keep, in_hbm(memory), gate, in_hbm(begun),
    )

    outgoing = call(
        project_body, shaped((devices, (CAPACITY + 1) * columns), BF16), [VMEM_SPEC] * 3
    )(gated_rows, mixer_out.T, take)
    incoming = exchange(outgoing)

    back, middle = call(
        expert_body,
        (shaped((devices, width), BF16), shaped((1, width))),
        [VMEM_SPEC] * 6 + [HBM_SPEC] * 3,
        [
            pltpu.VMEM((width - early_rows, hidden_dim), BF16),
            pltpu.VMEM((width, hidden_dim), BF16),
            pltpu.VMEM((hidden_dim, width), BF16),
            pltpu.VMEM((pl.cdiv((CAPACITY + 1) * columns, LANES), devices, LANES), F32),
            pltpu.VMEM((SLOTS * tiles, LANES), F32),
            pltpu.SemaphoreType.DMA((3, 4)),
        ],
        limit=24 * MIB,
    )(
        incoming, rows, mine, spread, expert_gain[None], early, gate,
        in_hbm(expert_up.reshape(width, hidden_dim)),
        in_hbm(expert_down.reshape(hidden_dim, width)),
    )
    returned = exchange(back)
    layer_out = call(finish_body, shaped((1, width), BF16), [VMEM_SPEC] * 3)(returned, weights, middle)
    return (layer_out, next_matrix[None], next_norm[None], next_max)


def solution(mesh):
    placed = (
        P("ep", None),
        P(),
        P(None, "ep"),
        P(None, "ep"),
        P(None, "ep"),
        P(None, "ep"),
        P(),
        P(),
        P(),
        P("ep", None, None, None),
        P("ep", None, None),
        P("ep", None),
        P(None, "ep"),
        P(),
        P("ep", None, None),
        P("ep", None, None),
        P("ep", None, None),
        P("ep"),
        P("ep", None),
        P("ep"),
        P("ep", None),
    )
    return jax.shard_map(
        local,
        mesh=mesh,
        in_specs=placed,
        out_specs=(P("ep", None), P("ep", None, None, None), P("ep", None, None), P("ep", None)),
        check_vma=False,
    )
```

```python
import functools

import jax
import jax.numpy as jnp
from jax import lax
from jax.experimental import pallas as pl
from jax.experimental.pallas import tpu as pltpu
from jax.sharding import PartitionSpec as P

GROUPS = 4
CAPACITY = 4
LANES = 128
SLOTS = 8
MIB = 1 << 20
AHEAD = 2_000_000_000
F32 = jnp.float32
BF16 = jnp.bfloat16
NT = (((1,), (1,)), ((), ()))


norm_eps = 1e-06


def root_norm(values, gain):
    return values * lax.rsqrt(jnp.mean(values * values, axis=-1, keepdims=True) + norm_eps) * gain


def exchange(blocks):
    count, width = blocks.shape
    halves = blocks.reshape(count, 2, width // 2)
    return lax.all_to_all(halves, "ep", split_axis=0, concat_axis=0, tiled=True).reshape(count, width)


VMEM_SPEC = pl.BlockSpec(memory_space=pltpu.VMEM)
SMEM_SPEC = pl.BlockSpec(memory_space=pltpu.SMEM)
HBM_SPEC = pl.BlockSpec(memory_space=pltpu.HBM)


def call(body, outs, ins, scratch=(), outputs=None, aliases={}, limit=8 * MIB, flops=10_000_000, moved=1_000_000):
    return pl.pallas_call(
        body,
        out_shape=outs,
        in_specs=ins,
        out_specs=outputs or jax.tree.map(lambda _: VMEM_SPEC, outs),
        scratch_shapes=scratch,
        input_output_aliases=aliases,
        compiler_params=pltpu.CompilerParams(vmem_limit_bytes=limit),
        cost_estimate=pl.CostEstimate(flops=flops, bytes_accessed=moved, transcendentals=0),
    )


def in_hbm(array):
    return pltpu.with_memory_space_constraint(array, pltpu.HBM)


def shaped(shape, dtype=F32):
    return jax.ShapeDtypeStruct(shape, dtype)


def feature_rows(ref, offset, columns):
    group = LANES // columns
    count = ref.shape[1] // group
    tile, lane = divmod(offset, LANES)
    pieces = [
        ref[tile, pl.ds(g, count, stride=group), :][:, lane:lane + columns] for g in range(group)
    ]
    return jnp.concatenate(pieces, axis=1)


def spill(ref, values):
    for t in range(ref.shape[0]):
        part = values[:, t * LANES:(t + 1) * LANES]
        ref[t, :, :part.shape[1]] = part


def own_number(parts_ref):
    ids = parts_ref[:, parts_ref.shape[1] - LANES:].astype(F32)
    lane = lax.broadcasted_iota(jnp.int32, ids.shape, 1)
    column = jnp.sum(jnp.where(lane == LANES - 1, ids, 0.0), axis=1, keepdims=True)
    return column[:1].astype(jnp.int32)


def diagonal(n):
    i = lax.broadcasted_iota(jnp.int32, (n, n), 0)
    j = lax.broadcasted_iota(jnp.int32, (n, n), 1)
    return i == j


def to_column(row):
    n = row.shape[1]
    spread = jnp.broadcast_to(row, (n, n))
    return jnp.sum(jnp.where(diagonal(n), spread, 0.0), axis=1, keepdims=True)


def to_row(col):
    n = col.shape[0]
    spread = jnp.broadcast_to(col, (n, n))
    return jnp.sum(jnp.where(diagonal(n), spread, 0.0), axis=0, keepdims=True)


def group_body(group_ref, out_ref):
    lane = lax.broadcasted_iota(jnp.int32, out_ref.shape, 1)
    out_ref[...] = jnp.where(lane == 0, group_ref[0], 0)


def spread_body(row_ref, group_ref, member_ref, member_weight_ref, out_ref, ids_ref, weights_ref):
    out_ref[...] = jnp.broadcast_to(row_ref[...].astype(F32), out_ref.shape).astype(BF16)
    lane = lax.broadcasted_iota(jnp.int32, ids_ref.shape, 1)
    ids = group_ref[...]
    weights = jnp.zeros(weights_ref.shape, F32)
    for k in range(member_ref.shape[1]):
        ids = jnp.where(lane == 1 + k, member_ref[:, k:k + 1], ids)
        weights = jnp.where(lane == 1 + k, member_weight_ref[:, k:k + 1], weights)
    ids_ref[...] = ids
    weights_ref[...] = weights


def columns_body(rows_ref, ids_ref, gain_ref, wq, wk, wv, wo, wi, wf, out_ref, pre_ref):
    heads = wi.shape[0]
    count = rows_ref.shape[0]
    normed = root_norm(rows_ref[...].astype(F32), gain_ref[...]).astype(BF16)
    stacked = jnp.concatenate([w[...] for w in (wq, wk, wv, wo)], axis=0)
    cols = lax.dot_general(normed, stacked, NT, preferred_element_type=F32).astype(BF16)
    total = cols.shape[1]
    out_ref[:, :total] = cols
    lane = lax.broadcasted_iota(jnp.int32, (count, LANES), 1)
    number = lax.broadcasted_iota(jnp.int32, (count, LANES), 0)
    ids = jnp.where(lane == LANES - 1, number, jnp.broadcast_to(ids_ref[...], (count, LANES)))
    out_ref[:, total:] = ids.astype(F32).astype(BF16)
    pre_ref[:heads, :] = lax.dot_general(wi[...], normed, NT, preferred_element_type=F32)
    pre_ref[heads:, :] = lax.dot_general(wf[...], normed, NT, preferred_element_type=F32)


def window_body(
    picks,
    group_weight, ids_ref, weights_ref, parts_ref, norm_ref, max_ref,
    value_ref, key_ref, keep_ref, mem_ref, gate_ref, begun_ref,
    take_ref, mine_ref, spread_ref, weight_ref, norm_out, max_out, early_ref, next_ref,
    old, new, sems,
):
    del begun_ref
    late = old.shape[0]
    first = next_ref.shape[0] - late
    loads = [
        pltpu.make_async_copy(mem_ref.at[first + h], old.at[h], sems.at[0, h]) for h in range(late)
    ]
    stores = [
        pltpu.make_async_copy(new.at[h], next_ref.at[first + h], sems.at[1, h]) for h in range(late)
    ]
    fetch = pltpu.make_async_copy(gate_ref.at[pl.ds(0, early_ref.shape[0])], early_ref, sems.at[0, late])
    for c in loads:
        c.start()
    fetch.start()
    norm_out[...] = norm_ref[...]
    max_out[...] = max_ref[...]
    slot_tables(
        group_weight, ids_ref, weights_ref, parts_ref, picks,
        take_ref, mine_ref, spread_ref, weight_ref,
    )
    turned = columns_of(value_ref[...])
    for h in range(late):
        row = slice(first + h, first + h + 1)
        loads[h].wait()
        new[h] = keep_ref[row] * old[h] + turned[:, row] * key_ref[row]
        stores[h].start()
    fetch.wait()
    for c in stores:
        c.wait()


def slot_tables(
    group_weight, local_ids, local_weights, parts_ref, picks,
    take_ref, mine_ref, spread_ref, weight_ref,
):
    count = parts_ref.shape[0]
    members = count // GROUPS
    me = own_number(parts_ref)
    ids = parts_ref[:, parts_ref.shape[1] - LANES:].astype(F32)
    lane = lax.broadcasted_iota(jnp.int32, ids.shape, 1)

    def row_of(k):
        return to_row(jnp.sum(jnp.where(lane == k, ids, 0.0), axis=1, keepdims=True))

    group = row_of(0)
    expert = lax.broadcasted_iota(jnp.int32, (count, count), 0)
    token = lax.broadcasted_iota(jnp.int32, (count, count), 1)
    hit = jnp.zeros((count, count), F32)
    column = lax.broadcasted_iota(jnp.int32, (count, 1), 0)
    weight = jnp.zeros((count, 1), F32)
    for k in range(picks):
        chosen = (group * members + row_of(1 + k)).astype(jnp.int32)
        hit = jnp.where(expert == chosen, 1.0, hit)
        local = local_ids[:, :1] * members + local_ids[:, 1 + k:2 + k]
        weight += jnp.where(column == local, group_weight[0] * local_weights[:, 1 + k:2 + k], 0.0)
    weight_ref[...] = weight
    upto = jnp.where(expert <= token, 1.0, 0.0).astype(BF16)
    place = jnp.dot(hit.astype(BF16), upto, preferred_element_type=F32)
    slot = lax.broadcasted_iota(jnp.int32, (SLOTS, count), 0)
    lane = lax.broadcasted_iota(jnp.int32, (count, SLOTS), 1)
    mine = jnp.zeros((SLOTS, count), F32)
    spread = jnp.zeros((count, SLOTS), F32)
    for s in range(CAPACITY + 1):
        if s < CAPACITY:
            take = jnp.where(place == s + 1.0, hit, 0.0)
        else:
            take = jnp.where(expert == token, 1.0, 0.0)
        take_ref[s] = take.astype(BF16)
        row = jnp.sum(jnp.where(expert == me, take, 0.0), axis=0, keepdims=True)
        mine = jnp.where(slot == s, row, mine)
        if s < CAPACITY:
            spread = jnp.where(lane == s, to_column(row), spread)
    mine_ref[...] = mine.astype(BF16)
    spread_ref[...] = spread.astype(BF16)


def cell_body(
    parts_ref, pre_ref, max_ref, bias_ref, norm_ref, mem_ref,
    gated_ref, norm_out, max_out, value_out, key_out, keep_out, next_ref,
    mem, new, wide, tall, sems,
):
    heads, head_dim = norm_ref.shape
    first = new.shape[0]
    copies = [pltpu.make_async_copy(mem_ref.at[h], mem.at[h], sems.at[0, h]) for h in range(heads)]
    stores = [pltpu.make_async_copy(new.at[h], next_ref.at[h], sems.at[1, h]) for h in range(first)]
    for c in copies:
        c.start()

    columns = (parts_ref.shape[1] - LANES) // 4
    tiles = head_dim // LANES
    rows = heads * tiles
    spill(wide, parts_ref[:, :4 * columns].astype(F32))
    for n in range(4):
        tall[n * rows:(n + 1) * rows, :] = feature_rows(wide, n * columns, columns)

    def heads_of(n):
        return jnp.concatenate(
            [tall[pl.ds(n * rows + p, heads, stride=tiles), :] for p in range(tiles)], axis=1
        )

    query, key, value, outgate = (heads_of(n) for n in range(4))
    key = key * head_dim ** (-0.5)

    pre = pre_ref[...]
    lane = lax.broadcasted_iota(jnp.int32, pre.shape, 1)
    pre = jnp.sum(jnp.where(lane == own_number(parts_ref), pre, 0.0), axis=1, keepdims=True)
    input_pre = pre[:heads]
    forget_pre = pre[heads:] + to_column(bias_ref[...])
    log_forget = jnp.minimum(forget_pre, 0.0) - jnp.log1p(jnp.exp(-jnp.abs(forget_pre)))
    carry = log_forget + to_column(max_ref[...])
    next_max = jnp.maximum(carry, input_pre)
    keep = jnp.exp(carry - next_max)
    admit = jnp.exp(input_pre - next_max)

    norm = norm_ref[...]
    score = admit * jnp.sum(key * query, axis=1, keepdims=True)
    denom = keep * jnp.sum(norm * query, axis=1, keepdims=True) + score
    scale = 1.0 / jnp.maximum(jnp.abs(denom), jnp.exp(-next_max))
    opened = jax.nn.sigmoid(outgate)
    norm_out[...] = keep * norm + admit * key
    max_out[...] = to_row(next_max)
    value_out[...] = admit * value
    key_out[...] = key
    keep_out[...] = jnp.broadcast_to(keep, keep_out.shape)

    count = gated_ref.shape[0]
    ones = jnp.ones((8, LANES), BF16)
    turned = columns_of(admit * value)
    for h in range(heads):
        copies[h].wait()
        sums = []
        for r in range(0, head_dim, LANES):
            block = mem[h, r:r + LANES, :]
            product = block * query[h:h + 1]
            sums.append(sum(product[:, p * LANES:(p + 1) * LANES] for p in range(tiles)))
            if h < first:
                new[h, r:r + LANES, :] = (
                    keep[h:h + 1] * block + turned[r:r + LANES, h:h + 1] * key[h:h + 1]
                )
        if h < first:
            stores[h].start()
        sums = jnp.concatenate(sums, axis=0)
        high = sums.astype(BF16)
        low = (sums - high.astype(F32)).astype(BF16)
        carried = lax.dot_general(ones, high, NT, preferred_element_type=F32)
        carried = carried + lax.dot_general(ones, low, NT, preferred_element_type=F32)
        numer = keep[h:h + 1] * carried[:1] + score[h:h + 1] * value[h:h + 1]
        gated = numer * scale[h:h + 1] * opened[h:h + 1]
        gated_ref[:, h * head_dim:(h + 1) * head_dim] = jnp.broadcast_to(
            gated, (count, head_dim)
        ).astype(BF16)
    for c in stores:
        c.wait()


def columns_of(value):
    heads = value.shape[0]
    if heads < 8:
        value = jnp.concatenate([value, jnp.zeros((8 - heads, value.shape[1]), F32)], axis=0)
    return value.T


def project_body(gated_ref, weight_ref, take_ref, out_ref):
    proj = lax.dot_general(gated_ref[...], weight_ref[...], NT, preferred_element_type=F32).astype(BF16)
    blocks = [
        jnp.dot(take_ref[s], proj, preferred_element_type=F32) for s in range(take_ref.shape[0])
    ]
    out_ref[...] = jnp.concatenate(blocks, axis=1).astype(BF16)


def expert_body(
    in_ref, rows_ref, mine_ref, spread_ref, gain_ref, early_ref, gate_ref, up_ref, down_ref,
    out_ref, middle_ref,
    gate, up, down, wide, tall, sems,
):
    width, hidden_dim = gate_ref.shape
    steps = sems.shape[1]
    here = early_ref.shape[0] * steps // width
    wide_step = width // steps
    tall_step = hidden_dim // steps

    def chunk(n, src, dst, k, step, skip=0):
        return pltpu.make_async_copy(
            src.at[pl.ds(k * step, step)], dst.at[pl.ds(k * step - skip, step)], sems.at[n, k]
        )

    gates = [None] * here + [
        chunk(0, gate_ref, gate, k, wide_step, early_ref.shape[0]) for k in range(here, steps)
    ]
    ups = [chunk(1, up_ref, up, k, wide_step) for k in range(steps)]
    downs = [chunk(2, down_ref, down, k, tall_step) for k in range(steps)]
    for k in range(steps):
        ups[k].start()
        if k >= here:
            gates[k].start()
    for k in range(steps):
        downs[k].start()

    used = CAPACITY + 1
    columns = in_ref.shape[1] // used
    tiles = width // LANES
    spill(wide, in_ref[...].astype(F32))
    for s in range(used):
        tall[s * tiles:(s + 1) * tiles, :] = feature_rows(wide, s * columns, columns)
    tall[used * tiles:, :] = jnp.zeros((tall.shape[0] - used * tiles, LANES), F32)
    projected = jnp.concatenate(
        [tall[pl.ds(r, SLOTS, stride=tiles), :] for r in range(tiles)], axis=1
    )
    resid = jnp.dot(mine_ref[...], rows_ref[...], preferred_element_type=F32)
    middle = (resid + projected).astype(BF16).astype(F32)
    middle_ref[...] = middle[CAPACITY:CAPACITY + 1]
    left = root_norm(middle, gain_ref[...]).astype(BF16)

    gate_part = jnp.dot(left[:, :here * wide_step], early_ref[...], preferred_element_type=F32)
    up_part = jnp.zeros((SLOTS, hidden_dim), F32)
    for k in range(steps):
        part = slice(k * wide_step, (k + 1) * wide_step)
        ups[k].wait()
        up_part += jnp.dot(left[:, part], up[part, :], preferred_element_type=F32)
        if k >= here:
            gates[k].wait()
            block = gate[(k - here) * wide_step:(k - here + 1) * wide_step, :]
            gate_part += jnp.dot(left[:, part], block, preferred_element_type=F32)
    hidden = (gate_part / (1.0 + jnp.exp(-gate_part)) * up_part).astype(BF16)
    result = jnp.zeros((SLOTS, width), F32)
    for k in range(steps):
        part = slice(k * tall_step, (k + 1) * tall_step)
        downs[k].wait()
        result += jnp.dot(hidden[:, part], down[part, :], preferred_element_type=F32)
    out_ref[...] = jnp.dot(
        spread_ref[...], result.astype(BF16), preferred_element_type=F32
    ).astype(BF16)


def finish_body(returned_ref, weight_ref, middle_ref, out_ref):
    mixture = jnp.sum(weight_ref[...] * returned_ref[...].astype(F32), axis=0, keepdims=True)
    out_ref[...] = (middle_ref[...] + mixture).astype(BF16)


def local(
    tokens,
    mixer_gain,
    query_weight,
    key_weight,
    value_weight,
    outgate_weight,
    input_weight,
    forget_weight,
    forget_bias,
    memory_matrix,
    memory_norm,
    memory_max,
    mixer_out,
    expert_gain,
    expert_gate,
    expert_up,
    expert_down,
    route_group,
    route_member,
    group_weight,
    member_weight,
):
    devices = lax.axis_size("ep")
    width = tokens.shape[1]
    columns = query_weight.shape[1]
    heads, head_dim = memory_norm.shape[1:]
    hidden_dim = expert_gate.shape[2]
    assert tokens.shape[0] == 1 and expert_gate.shape[0] == 1

    picks = route_member.shape[1]
    assert devices <= 256

    group_row = call(group_body, shaped((1, LANES), jnp.int32), [SMEM_SPEC], flops=AHEAD)(route_group)
    row, ids, local_weights = call(
        spread_body,
        (shaped((devices, width), BF16), shaped((1, LANES), jnp.int32), shaped((1, LANES))),
        [VMEM_SPEC] * 4,
        flops=AHEAD,
    )(tokens, group_row, route_member, member_weight)
    rows = exchange(row)

    cols, pre = call(
        columns_body,
        (shaped((devices, 4 * columns + LANES), BF16), shaped((2 * heads, devices))),
        [VMEM_SPEC] * 9,
        flops=AHEAD,
    )(
        rows, ids, mixer_gain[None], query_weight.T, key_weight.T, value_weight.T, outgate_weight.T,
        input_weight.T, forget_weight.T,
    )
    parts = exchange(cols)

    memory = memory_matrix.reshape(heads, head_dim, head_dim)
    tiles = width // LANES
    first = heads // 2
    gated, next_norm, next_max, value, key, keep, begun = call(
        cell_body,
        (
            shaped((devices, width), BF16), shaped((heads, head_dim)), shaped((1, heads)),
            shaped((heads, head_dim)), shaped((heads, head_dim)), shaped((heads, head_dim)),
            shaped((heads, head_dim, head_dim)),
        ),
        [VMEM_SPEC] * 5 + [HBM_SPEC],
        [
            pltpu.VMEM((heads, head_dim, head_dim), F32),
            pltpu.VMEM((first, head_dim, head_dim), F32),
            pltpu.VMEM((pl.cdiv(4 * columns, LANES), devices, LANES), F32),
            pltpu.VMEM((4 * tiles, LANES), F32),
            pltpu.SemaphoreType.DMA((2, heads)),
        ],
        outputs=[VMEM_SPEC] * 6 + [HBM_SPEC],
        limit=16 * MIB,
        flops=AHEAD,
    )(
        parts, pre, memory_max, forget_bias[None], memory_norm.reshape(heads, head_dim),
        in_hbm(memory),
    )
    gated_rows = exchange(gated)

    gate = in_hbm(expert_gate.reshape(width, hidden_dim))
    early_rows = width // 2
    take, mine, spread, weights, next_norm, next_max, early, next_matrix = call(
        functools.partial(window_body, picks),
        (
            shaped((CAPACITY + 1, devices, devices), BF16), shaped((SLOTS, devices), BF16),
            shaped((devices, SLOTS), BF16), shaped((devices, 1)),
            shaped((heads, head_dim)), shaped((1, heads)), shaped((early_rows, hidden_dim), BF16),
            shaped((heads, head_dim, head_dim)),
        ),
        [SMEM_SPEC] + [VMEM_SPEC] * 8 + [HBM_SPEC] * 3,
        [
            pltpu.VMEM((heads - first, head_dim, head_dim), F32),
            pltpu.VMEM((heads - first, head_dim, head_dim), F32),
            pltpu.SemaphoreType.DMA((2, heads - first + 1)),
        ],
        outputs=[VMEM_SPEC] * 7 + [HBM_SPEC],
        aliases={11: 7},
        limit=16 * MIB,
    )(
        group_weight, ids, local_weights, parts, next_norm, next_max,
        value, key, keep, in_hbm(memory), gate, in_hbm(begun),
    )

    outgoing = call(
        project_body, shaped((devices, (CAPACITY + 1) * columns), BF16), [VMEM_SPEC] * 3
    )(gated_rows, mixer_out.T, take)
    incoming = exchange(outgoing)

    back, middle = call(
        expert_body,
        (shaped((devices, width), BF16), shaped((1, width))),
        [VMEM_SPEC] * 6 + [HBM_SPEC] * 3,
        [
            pltpu.VMEM((width - early_rows, hidden_dim), BF16),
            pltpu.VMEM((width, hidden_dim), BF16),
            pltpu.VMEM((hidden_dim, width), BF16),
            pltpu.VMEM((pl.cdiv((CAPACITY + 1) * columns, LANES), devices, LANES), F32),
            pltpu.VMEM((SLOTS * tiles, LANES), F32),
            pltpu.SemaphoreType.DMA((3, 4)),
        ],
        limit=24 * MIB,
    )(
        incoming, rows, mine, spread, expert_gain[None], early, gate,
        in_hbm(expert_up.reshape(width, hidden_dim)),
        in_hbm(expert_down.reshape(hidden_dim, width)),
    )
    returned = exchange(back)
    layer_out = call(finish_body, shaped((1, width), BF16), [VMEM_SPEC] * 3)(returned, weights, middle)
    return (layer_out, next_matrix[None], next_norm[None], next_max)


def solution(mesh):
    placed = (
        P("ep", None),
        P(),
        P(None, "ep"),
        P(None, "ep"),
        P(None, "ep"),
        P(None, "ep"),
        P(),
        P(),
        P(),
        P("ep", None, None, None),
        P("ep", None, None),
        P("ep", None),
        P(None, "ep"),
        P(),
        P("ep", None, None),
        P("ep", None, None),
        P("ep", None, None),
        P("ep"),
        P("ep", None),
        P("ep"),
        P("ep", None),
    )
    return jax.shard_map(
        local,
        mesh=mesh,
        in_specs=placed,
        out_specs=(P("ep", None), P("ep", None, None, None), P("ep", None, None), P("ep", None)),
        check_vma=False,
    )
```

```python
import functools

import jax
import jax.numpy as jnp
from jax import lax
from jax.experimental import pallas as pl
from jax.experimental.pallas import tpu as pltpu
from jax.sharding import PartitionSpec as P

GROUPS = 4
CAPACITY = 4
LANES = 128
SLOTS = 8
MIB = 1 << 20
AHEAD = 2_000_000_000
F32 = jnp.float32
BF16 = jnp.bfloat16
NT = (((1,), (1,)), ((), ()))


norm_eps = 1e-06


def root_norm(values, gain):
    return values * lax.rsqrt(jnp.mean(values * values, axis=-1, keepdims=True) + norm_eps) * gain


def exchange(blocks):
    count, width = blocks.shape
    return exchange_halves(blocks.reshape(count, 2, width // 2))


def exchange_halves(halves):
    count, _, half = halves.shape
    return lax.all_to_all(halves, "ep", split_axis=0, concat_axis=0, tiled=True).reshape(count, 2 * half)


def halves_of(row, count):
    half = row.shape[1] // 2
    pair = jnp.concatenate([row[:, :half], row[:, half:]], axis=0).astype(BF16)
    return jnp.broadcast_to(pair[None], (count, 2, half))


VMEM_SPEC = pl.BlockSpec(memory_space=pltpu.VMEM)
SMEM_SPEC = pl.BlockSpec(memory_space=pltpu.SMEM)
HBM_SPEC = pl.BlockSpec(memory_space=pltpu.HBM)


def call(body, outs, ins, scratch=(), outputs=None, aliases={}, limit=8 * MIB, flops=10_000_000, moved=1_000_000):
    return pl.pallas_call(
        body,
        out_shape=outs,
        in_specs=ins,
        out_specs=outputs or jax.tree.map(lambda _: VMEM_SPEC, outs),
        scratch_shapes=scratch,
        input_output_aliases=aliases,
        compiler_params=pltpu.CompilerParams(vmem_limit_bytes=limit),
        cost_estimate=pl.CostEstimate(flops=flops, bytes_accessed=moved, transcendentals=0),
    )


def in_hbm(array):
    return pltpu.with_memory_space_constraint(array, pltpu.HBM)


def shaped(shape, dtype=F32):
    return jax.ShapeDtypeStruct(shape, dtype)


def feature_rows(ref, offset, columns):
    group = LANES // columns
    count = ref.shape[1] // group
    tile, lane = divmod(offset, LANES)
    pieces = [
        ref[tile, pl.ds(g, count, stride=group), :][:, lane:lane + columns] for g in range(group)
    ]
    return jnp.concatenate(pieces, axis=1)


def spill(ref, values):
    for t in range(ref.shape[0]):
        part = values[:, t * LANES:(t + 1) * LANES]
        ref[t, :, :part.shape[1]] = part


def own_number(parts_ref):
    ids = parts_ref[:, parts_ref.shape[1] - LANES:].astype(F32)
    lane = lax.broadcasted_iota(jnp.int32, ids.shape, 1)
    column = jnp.sum(jnp.where(lane == LANES - 1, ids, 0.0), axis=1, keepdims=True)
    return column[:1].astype(jnp.int32)


def diagonal(n):
    i = lax.broadcasted_iota(jnp.int32, (n, n), 0)
    j = lax.broadcasted_iota(jnp.int32, (n, n), 1)
    return i == j


def to_column(row):
    n = row.shape[1]
    spread = jnp.broadcast_to(row, (n, n))
    return jnp.sum(jnp.where(diagonal(n), spread, 0.0), axis=1, keepdims=True)


def to_row(col):
    n = col.shape[0]
    spread = jnp.broadcast_to(col, (n, n))
    return jnp.sum(jnp.where(diagonal(n), spread, 0.0), axis=0, keepdims=True)


def group_body(group_ref, out_ref):
    lane = lax.broadcasted_iota(jnp.int32, out_ref.shape, 1)
    out_ref[...] = jnp.where(lane == 0, group_ref[0], 0)


def spread_body(row_ref, group_ref, member_ref, member_weight_ref, out_ref, ids_ref, weights_ref):
    out_ref[...] = halves_of(row_ref[...].astype(F32), out_ref.shape[0])
    lane = lax.broadcasted_iota(jnp.int32, ids_ref.shape, 1)
    ids = group_ref[...]
    weights = jnp.zeros(weights_ref.shape, F32)
    for k in range(member_ref.shape[1]):
        ids = jnp.where(lane == 1 + k, member_ref[:, k:k + 1], ids)
        weights = jnp.where(lane == 1 + k, member_weight_ref[:, k:k + 1], weights)
    ids_ref[...] = ids
    weights_ref[...] = weights


def columns_body(rows_ref, ids_ref, gain_ref, wq, wk, wv, wo, wi, wf, out_ref, pre_ref):
    heads = wi.shape[0]
    count = rows_ref.shape[0]
    normed = root_norm(rows_ref[...].astype(F32), gain_ref[...]).astype(BF16)
    stacked = jnp.concatenate([w[...] for w in (wq, wk, wv, wo)], axis=0)
    cols = lax.dot_general(normed, stacked, NT, preferred_element_type=F32).astype(BF16)
    total = cols.shape[1]
    out_ref[:, :total] = cols
    lane = lax.broadcasted_iota(jnp.int32, (count, LANES), 1)
    number = lax.broadcasted_iota(jnp.int32, (count, LANES), 0)
    ids = jnp.where(lane == LANES - 1, number, jnp.broadcast_to(ids_ref[...], (count, LANES)))
    out_ref[:, total:] = ids.astype(F32).astype(BF16)
    pre_ref[:heads, :] = lax.dot_general(wi[...], normed, NT, preferred_element_type=F32)
    pre_ref[heads:, :] = lax.dot_general(wf[...], normed, NT, preferred_element_type=F32)


def window_body(
    picks,
    group_weight, ids_ref, weights_ref, parts_ref, norm_ref, max_ref,
    value_ref, key_ref, keep_ref, mem_ref, gate_ref, begun_ref,
    take_ref, mine_ref, spread_ref, weight_ref, norm_out, max_out, early_ref, next_ref,
    old, new, sems,
):
    del begun_ref
    late = old.shape[0]
    first = next_ref.shape[0] - late
    loads = [
        pltpu.make_async_copy(mem_ref.at[first + h], old.at[h], sems.at[0, h]) for h in range(late)
    ]
    stores = [
        pltpu.make_async_copy(new.at[h], next_ref.at[first + h], sems.at[1, h]) for h in range(late)
    ]
    fetch = pltpu.make_async_copy(gate_ref.at[pl.ds(0, early_ref.shape[0])], early_ref, sems.at[0, late])
    for c in loads:
        c.start()
    fetch.start()
    norm_out[...] = norm_ref[...]
    max_out[...] = max_ref[...]
    slot_tables(
        group_weight, ids_ref, weights_ref, parts_ref, picks,
        take_ref, mine_ref, spread_ref, weight_ref,
    )
    turned = columns_of(value_ref[...])
    for h in range(late):
        row = slice(first + h, first + h + 1)
        loads[h].wait()
        new[h] = keep_ref[row] * old[h] + turned[:, row] * key_ref[row]
        stores[h].start()
    fetch.wait()
    for c in stores:
        c.wait()


def slot_tables(
    group_weight, local_ids, local_weights, parts_ref, picks,
    take_ref, mine_ref, spread_ref, weight_ref,
):
    count = parts_ref.shape[0]
    members = count // GROUPS
    me = own_number(parts_ref)
    ids = parts_ref[:, parts_ref.shape[1] - LANES:].astype(F32)
    lane = lax.broadcasted_iota(jnp.int32, ids.shape, 1)

    def row_of(k):
        return to_row(jnp.sum(jnp.where(lane == k, ids, 0.0), axis=1, keepdims=True))

    group = row_of(0)
    expert = lax.broadcasted_iota(jnp.int32, (count, count), 0)
    token = lax.broadcasted_iota(jnp.int32, (count, count), 1)
    hit = jnp.zeros((count, count), F32)
    column = lax.broadcasted_iota(jnp.int32, (count, 1), 0)
    weight = jnp.zeros((count, 1), F32)
    for k in range(picks):
        chosen = (group * members + row_of(1 + k)).astype(jnp.int32)
        hit = jnp.where(expert == chosen, 1.0, hit)
        local = local_ids[:, :1] * members + local_ids[:, 1 + k:2 + k]
        weight += jnp.where(column == local, group_weight[0] * local_weights[:, 1 + k:2 + k], 0.0)
    weight_ref[...] = weight
    upto = jnp.where(expert <= token, 1.0, 0.0).astype(BF16)
    place = jnp.dot(hit.astype(BF16), upto, preferred_element_type=F32)
    slot = lax.broadcasted_iota(jnp.int32, (SLOTS, count), 0)
    lane = lax.broadcasted_iota(jnp.int32, (count, SLOTS), 1)
    mine = jnp.zeros((SLOTS, count), F32)
    spread = jnp.zeros((count, SLOTS), F32)
    for s in range(CAPACITY + 1):
        if s < CAPACITY:
            take = jnp.where(place == s + 1.0, hit, 0.0)
        else:
            take = jnp.where(expert == token, 1.0, 0.0)
        take_ref[s] = take.astype(BF16)
        row = jnp.sum(jnp.where(expert == me, take, 0.0), axis=0, keepdims=True)
        mine = jnp.where(slot == s, row, mine)
        if s < CAPACITY:
            spread = jnp.where(lane == s, to_column(row), spread)
    mine_ref[...] = mine.astype(BF16)
    spread_ref[...] = spread.astype(BF16)


def cell_body(
    parts_ref, pre_ref, max_ref, bias_ref, norm_ref, mem_ref,
    gated_ref, norm_out, max_out, value_out, key_out, keep_out, next_ref,
    mem, new, wide, tall, sems,
):
    heads, head_dim = norm_ref.shape
    first = new.shape[0]
    parts_of = sems.shape[2]
    rows_of = head_dim // parts_of
    copies = [
        [
            pltpu.make_async_copy(
                mem_ref.at[h, pl.ds(k * rows_of, rows_of)], mem.at[h, pl.ds(k * rows_of, rows_of)],
                sems.at[0, h, k],
            )
            for k in range(parts_of)
        ]
        for h in range(heads)
    ]
    stores = [pltpu.make_async_copy(new.at[h], next_ref.at[h], sems.at[1, h, 0]) for h in range(first)]
    for c in sum(copies, []):
        c.start()

    columns = (parts_ref.shape[1] - LANES) // 4
    tiles = head_dim // LANES
    rows = heads * tiles
    spill(wide, parts_ref[:, :4 * columns].astype(F32))
    for n in range(4):
        tall[n * rows:(n + 1) * rows, :] = feature_rows(wide, n * columns, columns)

    def heads_of(n):
        return jnp.concatenate(
            [tall[pl.ds(n * rows + p, heads, stride=tiles), :] for p in range(tiles)], axis=1
        )

    query, key, value, outgate = (heads_of(n) for n in range(4))
    key = key * head_dim ** (-0.5)

    pre = pre_ref[...]
    lane = lax.broadcasted_iota(jnp.int32, pre.shape, 1)
    pre = jnp.sum(jnp.where(lane == own_number(parts_ref), pre, 0.0), axis=1, keepdims=True)
    input_pre = pre[:heads]
    forget_pre = pre[heads:] + to_column(bias_ref[...])
    log_forget = jnp.minimum(forget_pre, 0.0) - jnp.log1p(jnp.exp(-jnp.abs(forget_pre)))
    carry = log_forget + to_column(max_ref[...])
    next_max = jnp.maximum(carry, input_pre)
    keep = jnp.exp(carry - next_max)
    admit = jnp.exp(input_pre - next_max)

    norm = norm_ref[...]
    score = admit * jnp.sum(key * query, axis=1, keepdims=True)
    denom = keep * jnp.sum(norm * query, axis=1, keepdims=True) + score
    scale = 1.0 / jnp.maximum(jnp.abs(denom), jnp.exp(-next_max))
    opened = jax.nn.sigmoid(outgate)
    norm_out[...] = keep * norm + admit * key
    max_out[...] = to_row(next_max)
    value_out[...] = admit * value
    key_out[...] = key
    keep_out[...] = jnp.broadcast_to(keep, keep_out.shape)

    outs = []
    ones = jnp.ones((8, LANES), BF16)
    turned = columns_of(admit * value)
    for h in range(heads):
        sums = []
        for r in range(0, head_dim, LANES):
            if r % rows_of == 0:
                copies[h][r // rows_of].wait()
            block = mem[h, r:r + LANES, :]
            product = block * query[h:h + 1]
            sums.append(sum(product[:, p * LANES:(p + 1) * LANES] for p in range(tiles)))
            if h < first:
                new[h, r:r + LANES, :] = (
                    keep[h:h + 1] * block + turned[r:r + LANES, h:h + 1] * key[h:h + 1]
                )
        if h < first:
            stores[h].start()
        sums = jnp.concatenate(sums, axis=0)
        high = sums.astype(BF16)
        low = (sums - high.astype(F32)).astype(BF16)
        carried = lax.dot_general(ones, high, NT, preferred_element_type=F32)
        carried = carried + lax.dot_general(ones, low, NT, preferred_element_type=F32)
        numer = keep[h:h + 1] * carried[:1] + score[h:h + 1] * value[h:h + 1]
        gated = numer * scale[h:h + 1] * opened[h:h + 1]
        outs.append(gated)
    gated_ref[...] = halves_of(jnp.concatenate(outs, axis=1), gated_ref.shape[0])
    for c in stores:
        c.wait()


def columns_of(value):
    heads = value.shape[0]
    if heads < 8:
        value = jnp.concatenate([value, jnp.zeros((8 - heads, value.shape[1]), F32)], axis=0)
    return value.T


def project_body(gated_ref, weight_ref, take_ref, out_ref):
    proj = lax.dot_general(gated_ref[...], weight_ref[...], NT, preferred_element_type=F32).astype(BF16)
    blocks = [
        jnp.dot(take_ref[s], proj, preferred_element_type=F32) for s in range(take_ref.shape[0])
    ]
    out_ref[...] = jnp.concatenate(blocks, axis=1).astype(BF16)


def expert_body(
    in_ref, rows_ref, mine_ref, spread_ref, gain_ref, early_ref, gate_ref, up_ref, down_ref,
    out_ref, middle_ref,
    gate, up, down, wide, tall, sems,
):
    width, hidden_dim = gate_ref.shape
    steps = sems.shape[1]
    here = early_ref.shape[0] * steps // width
    wide_step = width // steps
    tall_step = hidden_dim // steps

    def chunk(n, src, dst, k, step, skip=0):
        return pltpu.make_async_copy(
            src.at[pl.ds(k * step, step)], dst.at[pl.ds(k * step - skip, step)], sems.at[n, k]
        )

    gates = [None] * here + [
        chunk(0, gate_ref, gate, k, wide_step, early_ref.shape[0]) for k in range(here, steps)
    ]
    ups = [chunk(1, up_ref, up, k, wide_step) for k in range(steps)]
    downs = [chunk(2, down_ref, down, k, tall_step) for k in range(steps)]
    for k in range(steps):
        ups[k].start()
        if k >= here:
            gates[k].start()
    for k in range(steps):
        downs[k].start()

    used = CAPACITY + 1
    columns = in_ref.shape[1] // used
    tiles = width // LANES
    spill(wide, in_ref[...].astype(F32))
    for s in range(used):
        tall[s * tiles:(s + 1) * tiles, :] = feature_rows(wide, s * columns, columns)
    tall[used * tiles:, :] = jnp.zeros((tall.shape[0] - used * tiles, LANES), F32)
    projected = jnp.concatenate(
        [tall[pl.ds(r, SLOTS, stride=tiles), :] for r in range(tiles)], axis=1
    )
    resid = jnp.dot(mine_ref[...], rows_ref[...], preferred_element_type=F32)
    middle = (resid + projected).astype(BF16).astype(F32)
    middle_ref[...] = middle[CAPACITY:CAPACITY + 1]
    left = root_norm(middle, gain_ref[...]).astype(BF16)

    gate_part = jnp.dot(left[:, :here * wide_step], early_ref[...], preferred_element_type=F32)
    up_part = jnp.zeros((SLOTS, hidden_dim), F32)
    for k in range(steps):
        part = slice(k * wide_step, (k + 1) * wide_step)
        ups[k].wait()
        up_part += jnp.dot(left[:, part], up[part, :], preferred_element_type=F32)
        if k >= here:
            gates[k].wait()
            block = gate[(k - here) * wide_step:(k - here + 1) * wide_step, :]
            gate_part += jnp.dot(left[:, part], block, preferred_element_type=F32)
    hidden = (gate_part / (1.0 + jnp.exp(-gate_part)) * up_part).astype(BF16)
    result = jnp.zeros((SLOTS, width), F32)
    for k in range(steps):
        part = slice(k * tall_step, (k + 1) * tall_step)
        downs[k].wait()
        result += jnp.dot(hidden[:, part], down[part, :], preferred_element_type=F32)
    out_ref[...] = jnp.dot(
        spread_ref[...], result.astype(BF16), preferred_element_type=F32
    ).astype(BF16)


def finish_body(returned_ref, weight_ref, middle_ref, out_ref):
    mixture = jnp.sum(weight_ref[...] * returned_ref[...].astype(F32), axis=0, keepdims=True)
    out_ref[...] = (middle_ref[...] + mixture).astype(BF16)


def local(
    tokens,
    mixer_gain,
    query_weight,
    key_weight,
    value_weight,
    outgate_weight,
    input_weight,
    forget_weight,
    forget_bias,
    memory_matrix,
    memory_norm,
    memory_max,
    mixer_out,
    expert_gain,
    expert_gate,
    expert_up,
    expert_down,
    route_group,
    route_member,
    group_weight,
    member_weight,
):
    devices = lax.axis_size("ep")
    width = tokens.shape[1]
    columns = query_weight.shape[1]
    heads, head_dim = memory_norm.shape[1:]
    hidden_dim = expert_gate.shape[2]
    assert tokens.shape[0] == 1 and expert_gate.shape[0] == 1

    picks = route_member.shape[1]
    assert devices <= 256

    group_row = call(group_body, shaped((1, LANES), jnp.int32), [SMEM_SPEC], flops=AHEAD)(route_group)
    row, ids, local_weights = call(
        spread_body,
        (shaped((devices, 2, width // 2), BF16), shaped((1, LANES), jnp.int32), shaped((1, LANES))),
        [VMEM_SPEC] * 4,
        flops=AHEAD,
    )(tokens, group_row, route_member, member_weight)
    rows = exchange_halves(row)

    cols, pre = call(
        columns_body,
        (shaped((devices, 4 * columns + LANES), BF16), shaped((2 * heads, devices))),
        [VMEM_SPEC] * 9,
        flops=AHEAD,
    )(
        rows, ids, mixer_gain[None], query_weight.T, key_weight.T, value_weight.T, outgate_weight.T,
        input_weight.T, forget_weight.T,
    )
    parts = exchange(cols)

    memory = memory_matrix.reshape(heads, head_dim, head_dim)
    tiles = width // LANES
    first = max(heads // 4, 1)
    gated, next_norm, next_max, value, key, keep, begun = call(
        cell_body,
        (
            shaped((devices, 2, width // 2), BF16), shaped((heads, head_dim)), shaped((1, heads)),
            shaped((heads, head_dim)), shaped((heads, head_dim)), shaped((heads, head_dim)),
            shaped((heads, head_dim, head_dim)),
        ),
        [VMEM_SPEC] * 5 + [HBM_SPEC],
        [
            pltpu.VMEM((heads, head_dim, head_dim), F32),
            pltpu.VMEM((first, head_dim, head_dim), F32),
            pltpu.VMEM((pl.cdiv(4 * columns, LANES), devices, LANES), F32),
            pltpu.VMEM((4 * tiles, LANES), F32),
            pltpu.SemaphoreType.DMA((2, heads, 2)),
        ],
        outputs=[VMEM_SPEC] * 6 + [HBM_SPEC],
        limit=16 * MIB,
        flops=AHEAD,
    )(
        parts, pre, memory_max, forget_bias[None], memory_norm.reshape(heads, head_dim),
        in_hbm(memory),
    )
    gated_rows = exchange_halves(gated)

    gate = in_hbm(expert_gate.reshape(width, hidden_dim))
    early_rows = width // 2
    take, mine, spread, weights, next_norm, next_max, early, next_matrix = call(
        functools.partial(window_body, picks),
        (
            shaped((CAPACITY + 1, devices, devices), BF16), shaped((SLOTS, devices), BF16),
            shaped((devices, SLOTS), BF16), shaped((devices, 1)),
            shaped((heads, head_dim)), shaped((1, heads)), shaped((early_rows, hidden_dim), BF16),
            shaped((heads, head_dim, head_dim)),
        ),
        [SMEM_SPEC] + [VMEM_SPEC] * 8 + [HBM_SPEC] * 3,
        [
            pltpu.VMEM((heads - first, head_dim, head_dim), F32),
            pltpu.VMEM((heads - first, head_dim, head_dim), F32),
            pltpu.SemaphoreType.DMA((2, heads - first + 1)),
        ],
        outputs=[VMEM_SPEC] * 7 + [HBM_SPEC],
        aliases={11: 7},
        limit=16 * MIB,
    )(
        group_weight, ids, local_weights, parts, next_norm, next_max,
        value, key, keep, in_hbm(memory), gate, in_hbm(begun),
    )

    outgoing = call(
        project_body, shaped((devices, (CAPACITY + 1) * columns), BF16), [VMEM_SPEC] * 3
    )(gated_rows, mixer_out.T, take)
    incoming = exchange(outgoing)

    back, middle = call(
        expert_body,
        (shaped((devices, width), BF16), shaped((1, width))),
        [VMEM_SPEC] * 6 + [HBM_SPEC] * 3,
        [
            pltpu.VMEM((width - early_rows, hidden_dim), BF16),
            pltpu.VMEM((width, hidden_dim), BF16),
            pltpu.VMEM((hidden_dim, width), BF16),
            pltpu.VMEM((pl.cdiv((CAPACITY + 1) * columns, LANES), devices, LANES), F32),
            pltpu.VMEM((SLOTS * tiles, LANES), F32),
            pltpu.SemaphoreType.DMA((3, 4)),
        ],
        limit=24 * MIB,
    )(
        incoming, rows, mine, spread, expert_gain[None], early, gate,
        in_hbm(expert_up.reshape(width, hidden_dim)),
        in_hbm(expert_down.reshape(hidden_dim, width)),
    )
    returned = exchange(back)
    layer_out = call(finish_body, shaped((1, width), BF16), [VMEM_SPEC] * 3)(returned, weights, middle)
    return (layer_out, next_matrix[None], next_norm[None], next_max)


def solution(mesh):
    placed = (
        P("ep", None),
        P(),
        P(None, "ep"),
        P(None, "ep"),
        P(None, "ep"),
        P(None, "ep"),
        P(),
        P(),
        P(),
        P("ep", None, None, None),
        P("ep", None, None),
        P("ep", None),
        P(None, "ep"),
        P(),
        P("ep", None, None),
        P("ep", None, None),
        P("ep", None, None),
        P("ep"),
        P("ep", None),
        P("ep"),
        P("ep", None),
    )
    return jax.shard_map(
        local,
        mesh=mesh,
        in_specs=placed,
        out_specs=(P("ep", None), P("ep", None, None, None), P("ep", None, None), P("ep", None)),
        check_vma=False,
    )
```

```python
import functools

import jax
import jax.numpy as jnp
from jax import lax
from jax.experimental import pallas as pl
from jax.experimental.pallas import tpu as pltpu
from jax.sharding import PartitionSpec as P

GROUPS = 4
CAPACITY = 4
LANES = 128
SLOTS = 8
MIB = 1 << 20
AHEAD = 2_000_000_000
F32 = jnp.float32
BF16 = jnp.bfloat16
NT = (((1,), (1,)), ((), ()))


norm_eps = 1e-06


def root_norm(values, gain):
    return values * lax.rsqrt(jnp.mean(values * values, axis=-1, keepdims=True) + norm_eps) * gain


def exchange(blocks):
    count, width = blocks.shape
    return exchange_halves(blocks.reshape(count, 2, width // 2))


def exchange_halves(halves):
    count, _, half = halves.shape
    return lax.all_to_all(halves, "ep", split_axis=0, concat_axis=0, tiled=True).reshape(count, 2 * half)


def halves_of(row, count):
    half = row.shape[1] // 2
    pair = jnp.concatenate([row[:, :half], row[:, half:]], axis=0).astype(BF16)
    return jnp.broadcast_to(pair[None], (count, 2, half))


VMEM_SPEC = pl.BlockSpec(memory_space=pltpu.VMEM)
SMEM_SPEC = pl.BlockSpec(memory_space=pltpu.SMEM)
HBM_SPEC = pl.BlockSpec(memory_space=pltpu.HBM)


def call(body, outs, ins, scratch=(), outputs=None, aliases={}, limit=8 * MIB, flops=10_000_000, moved=1_000_000):
    return pl.pallas_call(
        body,
        out_shape=outs,
        in_specs=ins,
        out_specs=outputs or jax.tree.map(lambda _: VMEM_SPEC, outs),
        scratch_shapes=scratch,
        input_output_aliases=aliases,
        compiler_params=pltpu.CompilerParams(vmem_limit_bytes=limit),
        cost_estimate=pl.CostEstimate(flops=flops, bytes_accessed=moved, transcendentals=0),
    )


def in_hbm(array):
    return pltpu.with_memory_space_constraint(array, pltpu.HBM)


def shaped(shape, dtype=F32):
    return jax.ShapeDtypeStruct(shape, dtype)


def feature_rows(ref, offset, columns):
    group = LANES // columns
    count = ref.shape[1] // group
    tile, lane = divmod(offset, LANES)
    pieces = [
        ref[tile, pl.ds(g, count, stride=group), :][:, lane:lane + columns] for g in range(group)
    ]
    return jnp.concatenate(pieces, axis=1)


def spill(ref, values):
    for t in range(ref.shape[0]):
        part = values[:, t * LANES:(t + 1) * LANES]
        ref[t, :, :part.shape[1]] = part


def own_number(parts_ref):
    ids = parts_ref[:, parts_ref.shape[1] - LANES:].astype(F32)
    lane = lax.broadcasted_iota(jnp.int32, ids.shape, 1)
    column = jnp.sum(jnp.where(lane == LANES - 1, ids, 0.0), axis=1, keepdims=True)
    return column[:1].astype(jnp.int32)


def diagonal(n):
    i = lax.broadcasted_iota(jnp.int32, (n, n), 0)
    j = lax.broadcasted_iota(jnp.int32, (n, n), 1)
    return i == j


def to_column(row):
    n = row.shape[1]
    spread = jnp.broadcast_to(row, (n, n))
    return jnp.sum(jnp.where(diagonal(n), spread, 0.0), axis=1, keepdims=True)


def to_row(col):
    n = col.shape[0]
    spread = jnp.broadcast_to(col, (n, n))
    return jnp.sum(jnp.where(diagonal(n), spread, 0.0), axis=0, keepdims=True)


def group_body(group_ref, out_ref):
    lane = lax.broadcasted_iota(jnp.int32, out_ref.shape, 1)
    out_ref[...] = jnp.where(lane == 0, group_ref[0], 0)


def spread_body(row_ref, group_ref, member_ref, member_weight_ref, out_ref, ids_ref, weights_ref):
    out_ref[...] = halves_of(row_ref[...].astype(F32), out_ref.shape[0])
    lane = lax.broadcasted_iota(jnp.int32, ids_ref.shape, 1)
    ids = group_ref[...]
    weights = jnp.zeros(weights_ref.shape, F32)
    for k in range(member_ref.shape[1]):
        ids = jnp.where(lane == 1 + k, member_ref[:, k:k + 1], ids)
        weights = jnp.where(lane == 1 + k, member_weight_ref[:, k:k + 1], weights)
    ids_ref[...] = ids
    weights_ref[...] = weights


def columns_body(rows_ref, ids_ref, gain_ref, wq, wk, wv, wo, wi, wf, out_ref, pre_ref):
    heads = wi.shape[0]
    count = rows_ref.shape[0]
    normed = root_norm(rows_ref[...].astype(F32), gain_ref[...]).astype(BF16)
    stacked = jnp.concatenate([w[...] for w in (wq, wk, wv, wo)], axis=0)
    cols = lax.dot_general(normed, stacked, NT, preferred_element_type=F32).astype(BF16)
    total = cols.shape[1]
    out_ref[:, :total] = cols
    lane = lax.broadcasted_iota(jnp.int32, (count, LANES), 1)
    number = lax.broadcasted_iota(jnp.int32, (count, LANES), 0)
    ids = jnp.where(lane == LANES - 1, number, jnp.broadcast_to(ids_ref[...], (count, LANES)))
    out_ref[:, total:] = ids.astype(F32).astype(BF16)
    pre_ref[:heads, :] = lax.dot_general(wi[...], normed, NT, preferred_element_type=F32)
    pre_ref[heads:, :] = lax.dot_general(wf[...], normed, NT, preferred_element_type=F32)


def window_body(
    picks,
    group_weight, ids_ref, weights_ref, parts_ref, norm_ref, max_ref,
    value_ref, key_ref, keep_ref, mem_ref, gate_ref, begun_ref,
    take_ref, mine_ref, spread_ref, weight_ref, norm_out, max_out, early_ref, next_ref,
    old, new, sems,
):
    del begun_ref
    late = old.shape[0]
    first = next_ref.shape[0] - late
    loads = [
        pltpu.make_async_copy(mem_ref.at[first + h], old.at[h], sems.at[0, h]) for h in range(late)
    ]
    stores = [
        pltpu.make_async_copy(new.at[h], next_ref.at[first + h], sems.at[1, h]) for h in range(late)
    ]
    fetch = pltpu.make_async_copy(gate_ref.at[pl.ds(0, early_ref.shape[0])], early_ref, sems.at[0, late])
    for c in loads:
        c.start()
    fetch.start()
    norm_out[...] = norm_ref[...]
    max_out[...] = max_ref[...]
    slot_tables(
        group_weight, ids_ref, weights_ref, parts_ref, picks,
        take_ref, mine_ref, spread_ref, weight_ref,
    )
    turned = columns_of(value_ref[...])
    for h in range(late):
        row = slice(first + h, first + h + 1)
        loads[h].wait()
        new[h] = keep_ref[row] * old[h] + turned[:, row] * key_ref[row]
        stores[h].start()
    fetch.wait()
    for c in stores:
        c.wait()


def slot_tables(
    group_weight, local_ids, local_weights, parts_ref, picks,
    take_ref, mine_ref, spread_ref, weight_ref,
):
    count = parts_ref.shape[0]
    members = count // GROUPS
    me = own_number(parts_ref)
    ids = parts_ref[:, parts_ref.shape[1] - LANES:].astype(F32)
    lane = lax.broadcasted_iota(jnp.int32, ids.shape, 1)

    def row_of(k):
        return to_row(jnp.sum(jnp.where(lane == k, ids, 0.0), axis=1, keepdims=True))

    group = row_of(0)
    expert = lax.broadcasted_iota(jnp.int32, (count, count), 0)
    token = lax.broadcasted_iota(jnp.int32, (count, count), 1)
    hit = jnp.zeros((count, count), F32)
    column = lax.broadcasted_iota(jnp.int32, (count, 1), 0)
    weight = jnp.zeros((count, 1), F32)
    for k in range(picks):
        chosen = (group * members + row_of(1 + k)).astype(jnp.int32)
        hit = jnp.where(expert == chosen, 1.0, hit)
        local = local_ids[:, :1] * members + local_ids[:, 1 + k:2 + k]
        weight += jnp.where(column == local, group_weight[0] * local_weights[:, 1 + k:2 + k], 0.0)
    weight_ref[...] = weight
    upto = jnp.where(expert <= token, 1.0, 0.0).astype(BF16)
    place = jnp.dot(hit.astype(BF16), upto, preferred_element_type=F32)
    slot = lax.broadcasted_iota(jnp.int32, (SLOTS, count), 0)
    lane = lax.broadcasted_iota(jnp.int32, (count, SLOTS), 1)
    mine = jnp.zeros((SLOTS, count), F32)
    spread = jnp.zeros((count, SLOTS), F32)
    for s in range(CAPACITY + 1):
        if s < CAPACITY:
            take = jnp.where(place == s + 1.0, hit, 0.0)
        else:
            take = jnp.where(expert == token, 1.0, 0.0)
        take_ref[s] = take.astype(BF16)
        row = jnp.sum(jnp.where(expert == me, take, 0.0), axis=0, keepdims=True)
        mine = jnp.where(slot == s, row, mine)
        if s < CAPACITY:
            spread = jnp.where(lane == s, to_column(row), spread)
    mine_ref[...] = mine.astype(BF16)
    spread_ref[...] = spread


def cell_body(
    parts_ref, pre_ref, max_ref, bias_ref, norm_ref, mem_ref,
    gated_ref, norm_out, max_out, value_out, key_out, keep_out, next_ref,
    mem, new, wide, tall, sems,
):
    heads, head_dim = norm_ref.shape
    first = new.shape[0]
    parts_of = sems.shape[2]
    rows_of = head_dim // parts_of
    copies = [
        [
            pltpu.make_async_copy(
                mem_ref.at[h, pl.ds(k * rows_of, rows_of)], mem.at[h, pl.ds(k * rows_of, rows_of)],
                sems.at[0, h, k],
            )
            for k in range(parts_of)
        ]
        for h in range(heads)
    ]
    stores = [pltpu.make_async_copy(new.at[h], next_ref.at[h], sems.at[1, h, 0]) for h in range(first)]
    for c in sum(copies, []):
        c.start()

    columns = (parts_ref.shape[1] - LANES) // 4
    tiles = head_dim // LANES
    rows = heads * tiles
    spill(wide, parts_ref[:, :4 * columns].astype(F32))
    for n in range(4):
        tall[n * rows:(n + 1) * rows, :] = feature_rows(wide, n * columns, columns)

    def heads_of(n):
        return jnp.concatenate(
            [tall[pl.ds(n * rows + p, heads, stride=tiles), :] for p in range(tiles)], axis=1
        )

    query, key, value, outgate = (heads_of(n) for n in range(4))
    key = key * head_dim ** (-0.5)

    pre = pre_ref[...]
    lane = lax.broadcasted_iota(jnp.int32, pre.shape, 1)
    pre = jnp.sum(jnp.where(lane == own_number(parts_ref), pre, 0.0), axis=1, keepdims=True)
    input_pre = pre[:heads]
    forget_pre = pre[heads:] + to_column(bias_ref[...])
    log_forget = jnp.minimum(forget_pre, 0.0) - jnp.log1p(jnp.exp(-jnp.abs(forget_pre)))
    carry = log_forget + to_column(max_ref[...])
    next_max = jnp.maximum(carry, input_pre)
    keep = jnp.exp(carry - next_max)
    admit = jnp.exp(input_pre - next_max)

    norm = norm_ref[...]
    score = admit * jnp.sum(key * query, axis=1, keepdims=True)
    denom = keep * jnp.sum(norm * query, axis=1, keepdims=True) + score
    scale = 1.0 / jnp.maximum(jnp.abs(denom), jnp.exp(-next_max))
    opened = jax.nn.sigmoid(outgate)
    norm_out[...] = keep * norm + admit * key
    max_out[...] = to_row(next_max)
    value_out[...] = admit * value
    key_out[...] = key
    keep_out[...] = jnp.broadcast_to(keep, keep_out.shape)

    outs = []
    ones = jnp.ones((8, LANES), BF16)
    turned = columns_of(admit * value)
    for h in range(heads):
        sums = []
        for r in range(0, head_dim, LANES):
            if r % rows_of == 0:
                copies[h][r // rows_of].wait()
            block = mem[h, r:r + LANES, :]
            product = block * query[h:h + 1]
            sums.append(sum(product[:, p * LANES:(p + 1) * LANES] for p in range(tiles)))
            if h < first:
                new[h, r:r + LANES, :] = (
                    keep[h:h + 1] * block + turned[r:r + LANES, h:h + 1] * key[h:h + 1]
                )
        if h < first:
            stores[h].start()
        sums = jnp.concatenate(sums, axis=0)
        high = sums.astype(BF16)
        low = (sums - high.astype(F32)).astype(BF16)
        carried = lax.dot_general(ones, high, NT, preferred_element_type=F32)
        carried = carried + lax.dot_general(ones, low, NT, preferred_element_type=F32)
        numer = keep[h:h + 1] * carried[:1] + score[h:h + 1] * value[h:h + 1]
        gated = numer * scale[h:h + 1] * opened[h:h + 1]
        outs.append(gated)
    gated_ref[...] = halves_of(jnp.concatenate(outs, axis=1), gated_ref.shape[0])
    for c in stores:
        c.wait()


def columns_of(value):
    heads = value.shape[0]
    if heads < 8:
        value = jnp.concatenate([value, jnp.zeros((8 - heads, value.shape[1]), F32)], axis=0)
    return value.T


def project_body(gated_ref, weight_ref, take_ref, out_ref):
    proj = lax.dot_general(gated_ref[...], weight_ref[...], NT, preferred_element_type=F32).astype(BF16)
    blocks = [
        jnp.dot(take_ref[s], proj, preferred_element_type=F32) for s in range(take_ref.shape[0])
    ]
    out_ref[...] = jnp.concatenate(blocks, axis=1).astype(BF16)


def expert_body(
    in_ref, rows_ref, mine_ref, spread_ref, gain_ref, early_ref, gate_ref, up_ref, down_ref,
    out_ref, middle_ref,
    gate, up, down, wide, tall, sems,
):
    width, hidden_dim = gate_ref.shape
    steps = sems.shape[1] - 1
    here = early_ref.shape[0] * steps // width
    wide_step = width // steps
    tall_step = hidden_dim // steps

    def chunk(n, src, dst, k, step, skip=0):
        return pltpu.make_async_copy(
            src.at[pl.ds(k * step, step)], dst.at[pl.ds(k * step - skip, step)], sems.at[n, k]
        )

    gates = [None] * here + [
        chunk(0, gate_ref, gate, k, wide_step, early_ref.shape[0]) for k in range(here, steps)
    ]
    ups = [chunk(1, up_ref, up, k, wide_step) for k in range(steps)]
    cuts = [k * tall_step for k in range(steps)] + [hidden_dim - tall_step // 2, hidden_dim]
    downs = [
        pltpu.make_async_copy(down_ref.at[pl.ds(a, b - a)], down.at[pl.ds(a, b - a)], sems.at[2, k])
        for k, (a, b) in enumerate(zip(cuts, cuts[1:]))
    ]
    for k in range(steps):
        ups[k].start()
        if k >= here:
            gates[k].start()
    for c in downs:
        c.start()

    used = CAPACITY + 1
    columns = in_ref.shape[1] // used
    tiles = width // LANES
    spill(wide, in_ref[...].astype(F32))
    for s in range(used):
        tall[s * tiles:(s + 1) * tiles, :] = feature_rows(wide, s * columns, columns)
    tall[used * tiles:, :] = jnp.zeros((tall.shape[0] - used * tiles, LANES), F32)
    projected = jnp.concatenate(
        [tall[pl.ds(r, SLOTS, stride=tiles), :] for r in range(tiles)], axis=1
    )
    resid = jnp.dot(mine_ref[...], rows_ref[...], preferred_element_type=F32)
    middle = (resid + projected).astype(BF16).astype(F32)
    middle_ref[...] = middle[CAPACITY:CAPACITY + 1]
    left = root_norm(middle, gain_ref[...]).astype(BF16)

    gate_part = jnp.dot(left[:, :here * wide_step], early_ref[...], preferred_element_type=F32)
    up_part = jnp.zeros((SLOTS, hidden_dim), F32)
    for k in range(steps):
        part = slice(k * wide_step, (k + 1) * wide_step)
        ups[k].wait()
        up_part += jnp.dot(left[:, part], up[part, :], preferred_element_type=F32)
        if k >= here:
            gates[k].wait()
            block = gate[(k - here) * wide_step:(k - here + 1) * wide_step, :]
            gate_part += jnp.dot(left[:, part], block, preferred_element_type=F32)
    hidden = (gate_part / (1.0 + jnp.exp(-gate_part)) * up_part).astype(BF16)
    result = jnp.zeros((SLOTS, width), F32)
    for k, (a, b) in enumerate(zip(cuts, cuts[1:])):
        downs[k].wait()
        result += jnp.dot(hidden[:, a:b], down[a:b, :], preferred_element_type=F32)
    result = result.astype(BF16).astype(F32)
    spread = spread_ref[...]
    back = jnp.zeros(out_ref.shape, F32)
    for s in range(CAPACITY):
        back = jnp.where(spread[:, s:s + 1] > 0.5, result[s:s + 1], back)
    out_ref[...] = back.astype(BF16)


def finish_body(returned_ref, weight_ref, middle_ref, out_ref):
    mixture = jnp.sum(weight_ref[...] * returned_ref[...].astype(F32), axis=0, keepdims=True)
    out_ref[...] = (middle_ref[...] + mixture).astype(BF16)


def local(
    tokens,
    mixer_gain,
    query_weight,
    key_weight,
    value_weight,
    outgate_weight,
    input_weight,
    forget_weight,
    forget_bias,
    memory_matrix,
    memory_norm,
    memory_max,
    mixer_out,
    expert_gain,
    expert_gate,
    expert_up,
    expert_down,
    route_group,
    route_member,
    group_weight,
    member_weight,
):
    devices = lax.axis_size("ep")
    width = tokens.shape[1]
    columns = query_weight.shape[1]
    heads, head_dim = memory_norm.shape[1:]
    hidden_dim = expert_gate.shape[2]
    assert tokens.shape[0] == 1 and expert_gate.shape[0] == 1

    picks = route_member.shape[1]
    assert devices <= 256

    group_row = call(group_body, shaped((1, LANES), jnp.int32), [SMEM_SPEC], flops=AHEAD)(route_group)
    row, ids, local_weights = call(
        spread_body,
        (shaped((devices, 2, width // 2), BF16), shaped((1, LANES), jnp.int32), shaped((1, LANES))),
        [VMEM_SPEC] * 4,
        flops=AHEAD,
    )(tokens, group_row, route_member, member_weight)
    rows = exchange_halves(row)

    cols, pre = call(
        columns_body,
        (shaped((devices, 4 * columns + LANES), BF16), shaped((2 * heads, devices))),
        [VMEM_SPEC] * 9,
        flops=AHEAD,
    )(
        rows, ids, mixer_gain[None], query_weight.T, key_weight.T, value_weight.T, outgate_weight.T,
        input_weight.T, forget_weight.T,
    )
    parts = exchange(cols)

    memory = memory_matrix.reshape(heads, head_dim, head_dim)
    tiles = width // LANES
    first = max(heads // 4, 1)
    gated, next_norm, next_max, value, key, keep, begun = call(
        cell_body,
        (
            shaped((devices, 2, width // 2), BF16), shaped((heads, head_dim)), shaped((1, heads)),
            shaped((heads, head_dim)), shaped((heads, head_dim)), shaped((heads, head_dim)),
            shaped((heads, head_dim, head_dim)),
        ),
        [VMEM_SPEC] * 5 + [HBM_SPEC],
        [
            pltpu.VMEM((heads, head_dim, head_dim), F32),
            pltpu.VMEM((first, head_dim, head_dim), F32),
            pltpu.VMEM((pl.cdiv(4 * columns, LANES), devices, LANES), F32),
            pltpu.VMEM((4 * tiles, LANES), F32),
            pltpu.SemaphoreType.DMA((2, heads, 2)),
        ],
        outputs=[VMEM_SPEC] * 6 + [HBM_SPEC],
        limit=16 * MIB,
        flops=AHEAD,
    )(
        parts, pre, memory_max, forget_bias[None], memory_norm.reshape(heads, head_dim),
        in_hbm(memory),
    )
    gated_rows = exchange_halves(gated)

    gate = in_hbm(expert_gate.reshape(width, hidden_dim))
    early_rows = width // 2
    take, mine, spread, weights, next_norm, next_max, early, next_matrix = call(
        functools.partial(window_body, picks),
        (
            shaped((CAPACITY + 1, devices, devices), BF16), shaped((SLOTS, devices), BF16),
            shaped((devices, SLOTS)), shaped((devices, 1)),
            shaped((heads, head_dim)), shaped((1, heads)), shaped((early_rows, hidden_dim), BF16),
            shaped((heads, head_dim, head_dim)),
        ),
        [SMEM_SPEC] + [VMEM_SPEC] * 8 + [HBM_SPEC] * 3,
        [
            pltpu.VMEM((heads - first, head_dim, head_dim), F32),
            pltpu.VMEM((heads - first, head_dim, head_dim), F32),
            pltpu.SemaphoreType.DMA((2, heads - first + 1)),
        ],
        outputs=[VMEM_SPEC] * 7 + [HBM_SPEC],
        aliases={11: 7},
        limit=16 * MIB,
    )(
        group_weight, ids, local_weights, parts, next_norm, next_max,
        value, key, keep, in_hbm(memory), gate, in_hbm(begun),
    )

    outgoing = call(
        project_body, shaped((devices, (CAPACITY + 1) * columns), BF16), [VMEM_SPEC] * 3
    )(gated_rows, mixer_out.T, take)
    incoming = exchange(outgoing)

    back, middle = call(
        expert_body,
        (shaped((devices, width), BF16), shaped((1, width))),
        [VMEM_SPEC] * 6 + [HBM_SPEC] * 3,
        [
            pltpu.VMEM((width - early_rows, hidden_dim), BF16),
            pltpu.VMEM((width, hidden_dim), BF16),
            pltpu.VMEM((hidden_dim, width), BF16),
            pltpu.VMEM((pl.cdiv((CAPACITY + 1) * columns, LANES), devices, LANES), F32),
            pltpu.VMEM((SLOTS * tiles, LANES), F32),
            pltpu.SemaphoreType.DMA((3, 5)),
        ],
        limit=24 * MIB,
    )(
        incoming, rows, mine, spread, expert_gain[None], early, gate,
        in_hbm(expert_up.reshape(width, hidden_dim)),
        in_hbm(expert_down.reshape(hidden_dim, width)),
    )
    returned = exchange(back)
    layer_out = call(finish_body, shaped((1, width), BF16), [VMEM_SPEC] * 3)(returned, weights, middle)
    return (layer_out, next_matrix[None], next_norm[None], next_max)


def solution(mesh):
    placed = (
        P("ep", None),
        P(),
        P(None, "ep"),
        P(None, "ep"),
        P(None, "ep"),
        P(None, "ep"),
        P(),
        P(),
        P(),
        P("ep", None, None, None),
        P("ep", None, None),
        P("ep", None),
        P(None, "ep"),
        P(),
        P("ep", None, None),
        P("ep", None, None),
        P("ep", None, None),
        P("ep"),
        P("ep", None),
        P("ep"),
        P("ep", None),
    )
    return jax.shard_map(
        local,
        mesh=mesh,
        in_specs=placed,
        out_specs=(P("ep", None), P("ep", None, None, None), P("ep", None, None), P("ep", None)),
        check_vma=False,
    )
```
